32 devices in a mesh: fs: 8 (over z, x), tp: 4 (over y, core).
Axes of the slice: x: 2, y: 2, z: 4, core: 2. Of those that a mesh axis runs over, the one named last changes fastest.
Arguments:
- query_rows: bfloat16 [16384, 2048], P('fs', 'tp'), may hold values from -16 to 16
- key_rows: bfloat16 [16384, 2048], P('fs', 'tp'), may hold values from -8 to 8
- value_rows: bfloat16 [16384, 2048], P('fs', 'tp'), may hold values from -6 to 6
- mix_lambda: float32 [16], P('tp'), may hold values from 0.3 to 0.8
- head_gain: float32 [128], replicated, may hold values from 0.1 to 1.9
- out_cotangent: bfloat16 [16384, 2048], P('fs'), may hold values from -0.049804688 to 0.049804688
- layer_input: bfloat16 [16384, 2048], P('fs'), may hold values from -6 to 6
- value_cotangent: bfloat16 [16384, 2048], P('fs', 'tp'), may hold values from -0.049804688 to 0.049804688
- out_weight: float32 [2048, 2048], P('tp', 'fs'), may hold values from -0.125 to 0.125
- value_weight: float32 [2048, 2048], P('fs', 'tp'), may hold values from -0.125 to 0.125
- out_basis: bfloat16 [2048, 256], replicated, may hold values from -0.125 to 0.125
- value_basis: bfloat16 [2048, 256], replicated, may hold values from -0.125 to 0.125
- out_first: float32 [256, 2048], P('fs', 'tp'), may hold values from -20 to 20
- out_second: float32 [256, 2048], P('fs', 'tp'), may hold values from 0.02 to 0.5
- value_first: float32 [256, 2048], P('fs', 'tp'), may hold values from -20 to 20
- value_second: float32 [256, 2048], P('fs', 'tp'), may hold values from 0.02 to 0.5
Outputs:
- out_step: float32 [2048, 2048], P('tp', 'fs')
- value_step: float32 [2048, 2048], P('fs', 'tp')
- new_out_weight: float32 [2048, 2048], P('tp', 'fs')
- new_value_weight: float32 [2048, 2048], P('fs', 'tp')
- out_copy: bfloat16 [2048, 2048], P('tp')
- value_copy: bfloat16 [2048, 2048], P(None, 'tp')
- new_out_first: float32 [256, 2048], P('fs', 'tp')
- new_out_second: float32 [256, 2048], P('fs', 'tp')
- new_value_first: float32 [256, 2048], P('fs', 'tp')
- new_value_second: float32 [256, 2048], P('fs', 'tp')
The draws below stay inside these ranges and needn't reach their ends.
All inputs are finite; a program needn't handle non-finite values.
Results may differ from the reference program's by a relative error of at most 0.001.
Values may be sent and summed in bfloat16 or wider, within the bound.
No kernel may reach another device: no remote copies, remote signals or barrier semaphores. Data moves between devices by JAX's collectives and lax.ppermute only.
A program may use at most 192 MiB of HBM per device.

```python
import math
import jax
import jax.numpy as jnp
from jax import lax

D = 2048
H = 16
DH = 64
DV = 128
RANK = 256
LEN = 2048
TOKENS = 16384
V = 2048
QKW = 2048


def draw_query_rows(key, part):
    base_draw = jnp.clip(jax.random.normal(jax.random.fold_in(key, 1), (TOKENS // LEN, LEN, 2 * H, DH), jnp.float32) * 1.3, -5.2, 5.2)
    return jnp.clip(base_draw, -16.0, 16.0).reshape(TOKENS, QKW).astype(jnp.bfloat16)


def draw_key_rows(key, part):
    base_draw = jnp.clip(jax.random.normal(jax.random.fold_in(key, 2), (TOKENS // LEN, LEN, 2 * H, DH), jnp.float32) * 1.3, -5.2, 5.2)
    return jnp.clip(base_draw, -8.0, 8.0).reshape(TOKENS, QKW).astype(jnp.bfloat16)


def moment_draw(key, salt):
    row_rise = jnp.arange(RANK, dtype=jnp.float32)[:, None] / RANK
    col_rise = jnp.arange(V, dtype=jnp.float32)[None, :] / V
    jitter = jax.random.uniform(jax.random.fold_in(key, salt), (RANK, V), jnp.float32, -0.35, 0.35)
    scales = 0.3 * 10.0 ** (0.5 * (row_rise + col_rise)) * jnp.exp(jitter)
    values = jnp.clip(jax.random.normal(jax.random.fold_in(key, salt + 1), (RANK, V), jnp.float32), -4.0, 4.0)
    return jnp.clip(values * scales, -20.0, 20.0)


def draw_out_first(key, part):
    return moment_draw(key, 11)


def draw_value_first(key, part):
    return moment_draw(key, 21)


def shard_levels(key, shape, split, least, top_value):
    level = 1.0
    for axis_at, parts in split:
        heights = jax.random.uniform(jax.random.fold_in(jax.random.fold_in(key, 6), axis_at), (parts,), jnp.float32, least / len(split), top_value / len(split))
        level = level * jnp.repeat(jnp.exp(heights), shape[axis_at] // parts).reshape((-1,) + (1,) * (len(shape) - 1 - axis_at))
    return level


def scatter_about(key, shape, spread, reach, pieces=(), kind=jnp.bfloat16):
    drawn = jax.random.normal(key, shape, jnp.float32) * spread
    if len(pieces) > 0:
        drawn = shard_levels(key, shape, pieces, -0.22, 0.18) * drawn
    return jnp.clip(drawn, min=-reach, max=reach).astype(kind)


def setup_inputs(seed: int = 0) -> dict:
    key_list = jax.random.split(jax.random.key(seed), 17)
    return {
        "query_rows": draw_query_rows(jax.random.fold_in(key_list[16], 71), 0),
        "key_rows": draw_key_rows(jax.random.fold_in(key_list[16], 71), 0),
        "value_rows": scatter_about(key_list[2], (TOKENS, V), 1.0, 6.0, ((0, 8), (1, 4))),
        "mix_lambda": jnp.clip(0.3 + 0.5 * jax.random.uniform(key_list[3], (H,), jnp.float32) ** shard_levels(key_list[3], (H,), ((0, 4),), -0.2, 0.2), 0.3, 0.8),
        "head_gain": jnp.clip(1.0 + 0.18 * jax.random.normal(key_list[4], (DV,), jnp.float32), 0.1, 1.9),
        "out_cotangent": scatter_about(key_list[5], (TOKENS, D), 0.008, 0.049804688, ((0, 8),)),
        "layer_input": scatter_about(key_list[6], (TOKENS, D), 1.0, 6.0, ((0, 8),)),
        "value_cotangent": scatter_about(key_list[7], (TOKENS, V), 0.008, 0.049804688, ((0, 8), (1, 4))),
        "out_weight": scatter_about(key_list[8], (V, D), V ** -0.5, 0.125, ((0, 4), (1, 8)), jnp.float32),
        "value_weight": scatter_about(key_list[9], (D, V), D ** -0.5, 0.125, ((0, 8), (1, 4)), jnp.float32),
        "out_basis": scatter_about(key_list[10], (D, RANK), D ** -0.5, 0.125),
        "value_basis": scatter_about(key_list[11], (D, RANK), D ** -0.5, 0.125),
        "out_first": draw_out_first(jax.random.fold_in(key_list[16], 71), 0),
        "out_second": jnp.clip(jnp.exp(math.log(0.5) - 3.218876 * jax.random.uniform(key_list[13], (RANK, V), jnp.float32) ** shard_levels(key_list[13], (RANK, V), ((0, 8), (1, 4)), -0.2, 0.2)), 0.02, 0.5),
        "value_first": draw_value_first(jax.random.fold_in(key_list[16], 71), 0),
        "value_second": jnp.clip(jnp.exp(math.log(0.5) - 3.218876 * jax.random.uniform(key_list[15], (RANK, V), jnp.float32) ** shard_levels(key_list[15], (RANK, V), ((0, 8), (1, 4)), -0.2, 0.2)), 0.02, 0.5),
    }


EPSILON_NORM = 1e-05
EPSILON_ADAM = 1e-08
BETA_ONE = 0.9
BETA_TWO = 0.95
CLIP_RMS = 1.0
LEARN_RATE = 0.01

def moment_step(proj, first, second):
    new_first = BETA_ONE * first + (1.0 - BETA_ONE) * proj
    new_second = BETA_TWO * second + (1.0 - BETA_TWO) * proj * proj
    direction = new_first / (jnp.sqrt(new_second) + EPSILON_ADAM)
    return (new_first, new_second, direction)

def adapt(grad, basis, first, second):
    basis_wide = basis.astype(jnp.float32)
    proj = jnp.dot(basis_wide.T, grad, precision=lax.Precision.HIGHEST)
    new_first, new_second, direction = moment_step(proj, first, second)
    clip_factor = jnp.minimum(1.0, CLIP_RMS * math.sqrt(RANK * V) / jnp.sqrt(jnp.sum(direction * direction)))
    step_full = clip_factor * jnp.dot(basis_wide, direction, precision=lax.Precision.HIGHEST)
    return (step_full, new_first, new_second)

def reference(query_rows, key_rows, value_rows, mix_lambda, head_gain, out_cotangent, layer_input, value_cotangent, out_weight, value_weight, out_basis, value_basis, out_first, out_second, value_first, value_second):
    seq_count = TOKENS // LEN
    query_heads = query_rows.reshape(seq_count, LEN, H, 2, DH).transpose(0, 2, 3, 1, 4).reshape(seq_count * H, 2, LEN, DH)
    key_heads = key_rows.reshape(seq_count, LEN, H, 2, DH).transpose(0, 2, 3, 1, 4).reshape(seq_count * H, 2, LEN, DH)
    value_heads = value_rows.reshape(seq_count, LEN, H, DV).transpose(0, 2, 1, 3).reshape(seq_count * H, LEN, DV)
    lam_rows = jnp.tile(mix_lambda, seq_count)
    positions = jnp.arange(LEN)
    causal = positions[None, :] <= positions[:, None]

    def attend(operands):
        query_pair, key_pair, value_head, lam_value = operands
        scores = jnp.einsum('mqd,mkd->mqk', query_pair.astype(jnp.float32), key_pair.astype(jnp.float32)) * DH ** (-0.5)
        scores = jnp.where(causal[None], scores, -jnp.inf)
        row_peak = lax.optimization_barrier(jnp.max(scores, axis=-1, keepdims=True))
        exp_scores = jnp.exp(scores - row_peak)
        soft_maps = exp_scores / lax.optimization_barrier(jnp.sum(exp_scores, axis=-1, keepdims=True))
        mix_weights = (soft_maps[0] - lam_value * soft_maps[1]).astype(jnp.bfloat16)
        raw_out = jnp.dot(mix_weights, value_head, preferred_element_type=jnp.float32)
        normed = raw_out * lax.rsqrt(lax.optimization_barrier(jnp.mean(raw_out * raw_out, axis=-1, keepdims=True)) + EPSILON_NORM) * head_gain
        return normed.astype(jnp.bfloat16)
    head_blocks = lax.map(attend, (query_heads, key_heads, value_heads, lam_rows))
    head_out = head_blocks.reshape(seq_count, H, LEN, DV).transpose(0, 2, 1, 3).reshape(TOKENS, H * DV)
    out_grad = jnp.dot(out_cotangent.T, head_out, preferred_element_type=jnp.float32)
    value_grad = jnp.dot(layer_input.T, value_cotangent, preferred_element_type=jnp.float32)
    out_full, new_out_first, new_out_second = adapt(out_grad, out_basis, out_first, out_second)
    value_step, new_value_first, new_value_second = adapt(value_grad, value_basis, value_first, value_second)
    out_step = out_full.T
    new_out_weight = out_weight - LEARN_RATE * out_step
    new_value_weight = value_weight - LEARN_RATE * value_step
    return (out_step, value_step, new_out_weight, new_value_weight, new_out_weight.astype(jnp.bfloat16), new_value_weight.astype(jnp.bfloat16), new_out_first, new_out_second, new_value_first, new_value_second)
```

```python
import functools
import math

import jax
import jax.numpy as jnp
from jax import lax
from jax.experimental import pallas as pl
from jax.experimental.pallas import tpu as pltpu
from jax.sharding import PartitionSpec as P

DV = 128

EPSILON_NORM = 1e-05
EPSILON_ADAM = 1e-08
BETA_ONE = 0.9
BETA_TWO = 0.95
CLIP_RMS = 1.0
LEARN_RATE = 0.01
LOG2E = math.log2(math.e)

F32 = jnp.float32
BF16 = jnp.bfloat16
NT = (((1,), (1,)), ((), ()))
TN = (((0,), (0,)), ((), ()))
VMEM_BYTES = 60 * 2**20


def split_pair(x):
    high = x.astype(BF16)
    return high, (x - high.astype(F32)).astype(BF16)


def value_proj_kernel(x_ref, c_ref, basis_ref, proj_ref):
    y = jnp.dot(x_ref[...], basis_ref[...], preferred_element_type=F32)
    high, low = split_pair(y.T)
    part = jnp.dot(high, c_ref[...], preferred_element_type=F32) + jnp.dot(
        low, c_ref[...], preferred_element_type=F32
    )

    @pl.when(pl.program_id(0) == 0)
    def _():
        proj_ref[...] = part

    @pl.when(pl.program_id(0) > 0)
    def _():
        proj_ref[...] += part


def value_proj(x, c, basis):
    tokens, width = x.shape
    rank, cols = basis.shape[1], c.shape[1]
    block = min(256, tokens)
    return pl.pallas_call(
        value_proj_kernel,
        grid=(tokens // block,),
        out_shape=jax.ShapeDtypeStruct((rank, cols), F32),
        in_specs=[
            pl.BlockSpec((block, width), lambda t: (t, 0)),
            pl.BlockSpec((block, cols), lambda t: (t, 0)),
            pl.BlockSpec((width, rank), lambda t: (0, 0)),
        ],
        out_specs=pl.BlockSpec((rank, cols), lambda t: (0, 0)),
        cost_estimate=pl.CostEstimate(
            flops=2 * tokens * rank * (width + 2 * cols),
            bytes_accessed=2 * tokens * (width + cols),
            transcendentals=0,
        ),
        compiler_params=pltpu.CompilerParams(vmem_limit_bytes=VMEM_BYTES),
        name="value_proj",
    )(x, c, basis)


def low_rank_kernel(x_ref, basis_ref, high_ref, low_ref):
    y = jnp.dot(x_ref[...], basis_ref[...], preferred_element_type=F32)
    high, low = split_pair(y.T)
    high_ref[...] = high
    low_ref[...] = low


def low_rank_rows(x, basis):
    tokens, width = x.shape
    rank = basis.shape[1]
    block = min(256, tokens)
    out = jax.ShapeDtypeStruct((rank, tokens), BF16)
    return pl.pallas_call(
        low_rank_kernel,
        grid=(tokens // block,),
        out_shape=(out, out),
        in_specs=[
            pl.BlockSpec((block, width), lambda t: (t, 0)),
            pl.BlockSpec((width, rank), lambda t: (0, 0)),
        ],
        out_specs=[pl.BlockSpec((rank, block), lambda t: (0, t))] * 2,
        cost_estimate=pl.CostEstimate(
            flops=2 * tokens * rank * width,
            bytes_accessed=2 * tokens * width,
            transcendentals=0,
        ),
        compiler_params=pltpu.CompilerParams(vmem_limit_bytes=VMEM_BYTES),
        name="low_rank_rows",
    )(x, basis)


def attend_kernel(
    rows_at_once, lam_ref, gain_ref, q_ref, k_ref, v_ref, high_ref, low_ref,
    proj_ref, e_ref, h_ref, sum_ref,
):
    bq = rows_at_once
    seq, width = q_ref.shape
    half = width // 2
    lam = lam_ref[0]
    scale = half**-0.5
    first = lax.broadcasted_iota(jnp.int32, (1, width), 1) < half

    mark = (
        lax.broadcasted_iota(jnp.int32, (width, 128), 0) // half
        == lax.broadcasted_iota(jnp.int32, (width, 128), 1) // 64
    ).astype(BF16)

    def top_norm(ref):
        x = ref[...]
        return jnp.max(
            jnp.dot(x * x, mark, preferred_element_type=F32), axis=0, keepdims=True
        )

    bound = jnp.max(top_norm(q_ref) * top_norm(k_ref))
    small = bound < (70.0 / scale) ** 2

    def finish(base, mix, values):
        raw = jnp.dot(mix, values, preferred_element_type=F32)
        square = jnp.mean(raw * raw, axis=-1, keepdims=True)
        normed = raw * lax.rsqrt(square + EPSILON_NORM) * gain_ref[...]
        h_ref[pl.ds(base, bq), :] = normed.astype(BF16)

    @pl.when(small)
    def _():
        keep = lax.broadcasted_iota(jnp.int32, (bq, bq), 1) <= lax.broadcasted_iota(
            jnp.int32, (bq, bq), 0
        )
        keep_both = jnp.concatenate([keep, keep], axis=0)
        for i in range(seq // bq):
            slot = i % 2
            q = q_ref[i * bq : (i + 1) * bq, :]
            zero = jnp.zeros_like(q)
            both = jnp.concatenate(
                [jnp.where(first, q, zero), jnp.where(first, zero, q)], axis=0
            )
            for t in range(i + 1):
                scores = lax.dot_general(
                    both, k_ref[t * bq : (t + 1) * bq, :], NT, preferred_element_type=F32
                )
                e = jnp.exp2(scores * (scale * LOG2E))
                if t == i:
                    e = jnp.where(keep_both, e, 0.0)
                e_ref[slot, :, t * bq : (t + 1) * bq] = e
                part = e[:, :128]
                for c in range(1, bq // 128):
                    part = part + e[:, c * 128 : (c + 1) * 128]
                if t == 0:
                    sum_ref[slot] = part
                else:
                    sum_ref[slot] += part
            total = jnp.sum(sum_ref[slot], axis=-1, keepdims=True)
            one = 1.0 / total[:bq]
            two = lam / total[bq:]
            n = (i + 1) * bq
            mix = e_ref[slot, :bq, :n] * one - e_ref[slot, bq:, :n] * two
            finish(i * bq, mix.astype(BF16), v_ref[:n, :])

    @pl.when(jnp.logical_not(small))
    def _():
        def block(i, carry):
            base = i * bq
            q = q_ref[pl.ds(base, bq), :]
            zero = jnp.zeros_like(q)
            for m in range(2):
                picked = jnp.where(first if m == 0 else jnp.logical_not(first), q, zero)
                scores = (
                    lax.dot_general(picked, k_ref[...], NT, preferred_element_type=F32)
                    * scale
                )
                rows = base + lax.broadcasted_iota(jnp.int32, (bq, seq), 0)
                cols = lax.broadcasted_iota(jnp.int32, (bq, seq), 1)
                scores = jnp.where(cols <= rows, scores, -jnp.inf)
                e_ref[0, m * bq : (m + 1) * bq, :] = jnp.exp(
                    scores - jnp.max(scores, axis=-1, keepdims=True)
                )
            one = 1.0 / jnp.sum(e_ref[0, :bq, :], axis=-1, keepdims=True)
            two = lam / jnp.sum(e_ref[0, bq:, :], axis=-1, keepdims=True)
            mix = e_ref[0, :bq, :] * one - e_ref[0, bq:, :] * two
            finish(base, mix.astype(BF16), v_ref[...])
            return carry

        lax.fori_loop(0, seq // bq, block, 0)

    h = h_ref[...]
    proj_ref[...] = jnp.dot(high_ref[...], h, preferred_element_type=F32) + jnp.dot(
        low_ref[...], h, preferred_element_type=F32
    )


def attend_head(head, query_rows, key_rows, value_rows, mix_lambda, head_gain, high, low):
    seq = query_rows.shape[0]
    heads = mix_lambda.shape[0]
    width = query_rows.shape[1] // heads
    rank = high.shape[0]
    bq = min(256, seq)
    whole = lambda shape: pl.BlockSpec(shape, lambda i: (0, 0))
    own = lambda shape: pl.BlockSpec(shape, lambda i: (0, head))
    return pl.pallas_call(
        functools.partial(attend_kernel, bq),
        grid=(1,),
        out_shape=jax.ShapeDtypeStruct((rank, DV), F32),
        in_specs=[
            pl.BlockSpec(memory_space=pltpu.SMEM),
            whole((1, DV)),
            own((seq, width)),
            own((seq, width)),
            own((seq, DV)),
            whole((rank, seq)),
            whole((rank, seq)),
        ],
        out_specs=whole((rank, DV)),
        scratch_shapes=[
            pltpu.VMEM((2, 2 * bq, seq), F32),
            pltpu.VMEM((seq, DV), BF16),
            pltpu.VMEM((2, 2 * bq, 128), F32),
        ],
        cost_estimate=pl.CostEstimate(
            flops=8 * seq * seq * DV,
            bytes_accessed=2 * seq * (2 * width + DV + 2 * rank),
            transcendentals=seq * seq,
        ),
        compiler_params=pltpu.CompilerParams(vmem_limit_bytes=VMEM_BYTES),
        name="attend_head",
    )(
        lax.slice_in_dim(mix_lambda, head, head + 1),
        head_gain.reshape(1, DV),
        query_rows,
        key_rows,
        value_rows,
        high,
        low,
    )


def out_final_kernel(
    me_ref, clip_ref, dir_ref, basis_ref, near_ref, far_ref,
    copy_ref, step_ref, weight_ref, high_ref, low_ref,
):
    slot = pl.program_id(0)
    blocks = pl.num_programs(0)

    @pl.when(slot == 0)
    def _():
        high, low = split_pair(dir_ref[...].T)
        high_ref[...] = high
        low_ref[...] = low

    total = lax.dot_general(
        high_ref[...], basis_ref[...], NT, preferred_element_type=F32
    ) + lax.dot_general(low_ref[...], basis_ref[...], NT, preferred_element_type=F32)
    step = clip_ref[0] * total
    change = LEARN_RATE * step

    @pl.when(slot == 0)
    def _():
        weight = near_ref[0] - change
        step_ref[...] = step
        weight_ref[...] = weight
        copy_ref[...] = weight.astype(BF16)

    @pl.when((slot > 0) & (slot < blocks // 2))
    def _():
        copy_ref[...] = (near_ref[0] - change).astype(BF16)

    @pl.when(slot >= blocks // 2)
    def _():
        copy_ref[...] = (far_ref[0] - change).astype(BF16)


def out_final(me, clip, direction, basis, near, far):
    rank, cols = direction.shape
    half, _, share = near.shape
    width = basis.shape[0]

    def owner(s, me):
        return jnp.where(s < half, 2 * s, 2 * (s - half) + 1) ^ me[0]

    grid_spec = pltpu.PrefetchScalarGridSpec(
        num_scalar_prefetch=1,
        grid=(2 * half,),
        in_specs=[
            pl.BlockSpec(memory_space=pltpu.SMEM),
            pl.BlockSpec((rank, cols), lambda s, me: (0, 0)),
            pl.BlockSpec((share, rank), lambda s, me: (owner(s, me), 0)),
            pl.BlockSpec((1, cols, share), lambda s, me: (jnp.minimum(s, half - 1), 0, 0)),
            pl.BlockSpec((1, cols, share), lambda s, me: (jnp.maximum(s - half, 0), 0, 0)),
        ],
        out_specs=[
            pl.BlockSpec((cols, share), lambda s, me: (0, owner(s, me))),
            pl.BlockSpec((cols, share), lambda s, me: (0, 0)),
            pl.BlockSpec((cols, share), lambda s, me: (0, 0)),
        ],
        scratch_shapes=[pltpu.VMEM((cols, rank), BF16)] * 2,
    )
    block = jax.ShapeDtypeStruct((cols, share), F32)
    return pl.pallas_call(
        out_final_kernel,
        grid_spec=grid_spec,
        out_shape=(jax.ShapeDtypeStruct((cols, width), BF16), block, block),
        cost_estimate=pl.CostEstimate(
            flops=4 * rank * cols * width,
            bytes_accessed=6 * cols * width,
            transcendentals=0,
        ),
        compiler_params=pltpu.CompilerParams(vmem_limit_bytes=VMEM_BYTES),
        name="out_final",
    )(me.reshape(1), clip.reshape(1), direction, basis, near, far)


def value_final_kernel(clip_ref, dir_ref, basis_ref, old_ref, step_ref, weight_ref, copy_ref):
    high, low = split_pair(dir_ref[...])
    total = jnp.dot(basis_ref[...], high, preferred_element_type=F32) + jnp.dot(
        basis_ref[...], low, preferred_element_type=F32
    )
    step = clip_ref[0] * total
    weight = old_ref[...] - LEARN_RATE * step
    step_ref[...] = step
    weight_ref[...] = weight
    copy_ref[...] = weight.astype(BF16)


def value_final(clip, direction, basis_rows, old):
    block = jax.ShapeDtypeStruct(old.shape, F32)
    vmem = pl.BlockSpec(memory_space=pltpu.VMEM)
    return pl.pallas_call(
        value_final_kernel,
        out_shape=(block, block, jax.ShapeDtypeStruct(old.shape, BF16)),
        in_specs=[pl.BlockSpec(memory_space=pltpu.SMEM), vmem, vmem, vmem],
        out_specs=[vmem, vmem, vmem],
        cost_estimate=pl.CostEstimate(
            flops=4 * direction.size * old.shape[0],
            bytes_accessed=14 * old.size,
            transcendentals=0,
        ),
        name="value_final",
    )(clip.reshape(1), direction, basis_rows, old)


def swap(x, axis, bit):
    n = lax.axis_size(axis)
    return lax.ppermute(x, axis, [(i, i ^ bit) for i in range(n)])


def bits_down(n):
    bits = [1 << b for b in range(n.bit_length() - 1)]
    return bits[::-1]


def reduce_scatter(x, axis):
    n = lax.axis_size(axis)
    me = lax.axis_index(axis)
    rows, cols = x.shape
    bits = bits_down(n)
    x = x.reshape((2,) * len(bits) + (rows // n, cols))
    for bit in bits[::-1]:
        at = x.ndim - 3
        mine = (me // bit) % 2
        keep = lax.dynamic_index_in_dim(x, mine, at, keepdims=False)
        send = lax.dynamic_index_in_dim(x, 1 - mine, at, keepdims=False)
        x = keep + swap(send, axis, bit)
    return x


def all_gather(x, axis):
    n = lax.axis_size(axis)
    me = lax.axis_index(axis)
    rows, cols = x.shape
    for at, bit in enumerate(bits_down(n)):
        other = swap(x, axis, bit)
        mine = (me // bit) % 2
        x = jnp.where(
            mine == 0, jnp.stack([x, other], axis=at), jnp.stack([other, x], axis=at)
        )
    return x.reshape(n * rows, cols)


def gather_by_distance(x, axis):
    x = x[None]
    bits = bits_down(lax.axis_size(axis))
    for bit in bits[:-1]:
        other = swap(x, axis, bit)
        x = jnp.stack([x, other], axis=1).reshape((-1,) + x.shape[1:])
    return x, swap(x, axis, bits[-1])


def sum_over(x, axis):
    for bit in bits_down(lax.axis_size(axis))[::-1]:
        x = x + swap(x, axis, bit)
    return x


def moment_step(proj, first, second):
    new_first = BETA_ONE * first + (1.0 - BETA_ONE) * proj
    new_second = BETA_TWO * second + (1.0 - BETA_TWO) * proj * proj
    direction = new_first / (jnp.sqrt(new_second) + EPSILON_ADAM)
    return (new_first, new_second, direction)


def clip_of(direction):
    entry_count = direction.size * lax.axis_size("tp")
    total = sum_over(jnp.sum(direction * direction).reshape(1, 1), "tp")
    return jnp.minimum(1.0, CLIP_RMS * math.sqrt(entry_count) / jnp.sqrt(total))


def body(
    query_rows,
    key_rows,
    value_rows,
    mix_lambda,
    head_gain,
    out_cotangent,
    layer_input,
    value_cotangent,
    out_weight,
    value_weight,
    out_basis,
    value_basis,
    out_first,
    out_second,
    value_first,
    value_second,
):
    me = lax.axis_index("fs")
    near, far = gather_by_distance(out_weight, "fs")

    value_part = value_proj(layer_input, value_cotangent, value_basis)
    value_sum = reduce_scatter(value_part, "fs")
    new_value_first, new_value_second, value_dir = moment_step(
        value_sum, value_first, value_second
    )
    value_dir = all_gather(value_dir, "fs")
    share = value_weight.shape[0]
    basis_rows = lax.dynamic_slice_in_dim(value_basis, me * share, share, 0)
    value_step, new_value_weight, value_rounded = value_final(
        clip_of(value_dir), value_dir, basis_rows, value_weight
    )
    value_copy = all_gather(value_rounded, "fs")

    high, low = low_rank_rows(out_cotangent, out_basis)
    out_part = jnp.concatenate(
        [
            attend_head(h, query_rows, key_rows, value_rows, mix_lambda, head_gain, high, low)
            for h in range(mix_lambda.shape[0])
        ],
        axis=1,
    )
    out_sum = reduce_scatter(out_part, "fs")
    new_out_first, new_out_second, out_dir = moment_step(out_sum, out_first, out_second)
    out_dir = all_gather(out_dir, "fs")
    out_copy, out_step, new_out_weight = out_final(
        me, clip_of(out_dir), out_dir, out_basis, near, far
    )
    return (
        out_step,
        value_step,
        new_out_weight,
        new_value_weight,
        out_copy,
        value_copy,
        new_out_first,
        new_out_second,
        new_value_first,
        new_value_second,
    )


def solution(mesh):
    split, rows = P("fs", "tp"), P("fs", None)
    placed = (
        split, split, split, P("tp"), P(), rows, rows, split,
        P("tp", "fs"), split, P(), P(), split, split, split, split,
    )
    return jax.shard_map(
        body,
        mesh=mesh,
        in_specs=placed,
        out_specs=(
            P("tp", "fs"), split, P("tp", "fs"), split, P("tp", None), P(None, "tp"),
            split, split, split, split,
        ),
        check_vma=False,
    )
```

```python
import functools
import math

import jax
import jax.numpy as jnp
from jax import lax
from jax.experimental import pallas as pl
from jax.experimental.pallas import tpu as pltpu
from jax.sharding import PartitionSpec as P

DV = 128

EPSILON_NORM = 1e-05
EPSILON_ADAM = 1e-08
BETA_ONE = 0.9
BETA_TWO = 0.95
CLIP_RMS = 1.0
LEARN_RATE = 0.01
LOG2E = math.log2(math.e)

F32 = jnp.float32
BF16 = jnp.bfloat16
NT = (((1,), (1,)), ((), ()))
VMEM_BYTES = 60 * 2**20


def split_pair(x):
    high = x.astype(BF16)
    return high, (x - high.astype(F32)).astype(BF16)


def value_proj_kernel(x_ref, c_ref, basis_ref, proj_ref):
    y = jnp.dot(x_ref[...], basis_ref[...], preferred_element_type=F32)
    high, low = split_pair(y.T)
    part = jnp.dot(high, c_ref[...], preferred_element_type=F32) + jnp.dot(
        low, c_ref[...], preferred_element_type=F32
    )

    @pl.when(pl.program_id(0) == 0)
    def _():
        proj_ref[...] = part

    @pl.when(pl.program_id(0) > 0)
    def _():
        proj_ref[...] += part


def value_proj(x, c, basis):
    tokens, width = x.shape
    rank, cols = basis.shape[1], c.shape[1]
    block = min(512, tokens)
    return pl.pallas_call(
        value_proj_kernel,
        grid=(tokens // block,),
        out_shape=jax.ShapeDtypeStruct((rank, cols), F32),
        in_specs=[
            pl.BlockSpec((block, width), lambda t: (t, 0)),
            pl.BlockSpec((block, cols), lambda t: (t, 0)),
            pl.BlockSpec((width, rank), lambda t: (0, 0)),
        ],
        out_specs=pl.BlockSpec((rank, cols), lambda t: (0, 0)),
        cost_estimate=pl.CostEstimate(
            flops=2 * tokens * rank * (width + 2 * cols),
            bytes_accessed=2 * tokens * (width + cols),
            transcendentals=0,
        ),
        compiler_params=pltpu.CompilerParams(vmem_limit_bytes=VMEM_BYTES),
        name="value_proj",
    )(x, c, basis)


def low_rank_kernel(x_ref, basis_ref, high_ref, low_ref):
    y = jnp.dot(x_ref[...], basis_ref[...], preferred_element_type=F32)
    high, low = split_pair(y.T)
    high_ref[...] = high
    low_ref[...] = low


def low_rank_rows(half, x, basis):
    tokens, width = x.shape[0] // 2, x.shape[1]
    rank = basis.shape[1]
    block = min(512, tokens)
    skip = half * (tokens // block)
    out = jax.ShapeDtypeStruct((rank, tokens), BF16)
    return pl.pallas_call(
        low_rank_kernel,
        grid=(tokens // block,),
        out_shape=(out, out),
        in_specs=[
            pl.BlockSpec((block, width), lambda t: (t + skip, 0)),
            pl.BlockSpec((width, rank), lambda t: (0, 0)),
        ],
        out_specs=[pl.BlockSpec((rank, block), lambda t: (0, t))] * 2,
        cost_estimate=pl.CostEstimate(
            flops=2 * tokens * rank * width,
            bytes_accessed=2 * tokens * width,
            transcendentals=0,
        ),
        compiler_params=pltpu.CompilerParams(vmem_limit_bytes=VMEM_BYTES),
        name="low_rank_rows",
    )(x, basis)


def attend_kernel(
    bq, start, lam_ref, gain_ref, q_hbm, k_hbm, v_hbm, high_hbm, low_hbm, high_two,
    low_two, *rest
):
    proj_ref, q_all, k_all, v_all, high_ref, low_ref, e_ref, h_ref, sum_ref, sems, late_sems = (
        rest[-11:]
    )
    count, seq, width = q_all.shape
    step = pl.program_id(0)

    def head_copies(j):
        columns = pl.ds(pl.multiple_of((start + j) * width, width), width)
        return [
            pltpu.make_async_copy(source.at[:, columns], target.at[j], sems.at[j, i])
            for i, (source, target) in enumerate(
                ((k_hbm, k_all), (q_hbm, q_all), (v_hbm, v_all))
            )
        ]

    def late_copies():
        pairs = ((high_hbm, high_ref), (low_hbm, low_ref), (high_two, high_ref), (low_two, low_ref))
        return [
            pltpu.make_async_copy(
                source,
                target.at[:, pl.ds(i // 2 * (seq // 2), seq // 2)],
                late_sems.at[i],
            )
            for i, (source, target) in enumerate(pairs)
        ]

    @pl.when(step == 0)
    def _():
        for copy in head_copies(0):
            copy.start()
        for copy in late_copies():
            copy.start()
        for j in range(1, count):
            for copy in head_copies(j):
                copy.start()

    for copy in head_copies(step):
        copy.wait()
    q_ref, k_ref, v_ref = q_all.at[step], k_all.at[step], v_all.at[step]
    half = width // 2
    lam = lam_ref[start + step]
    scale = half**-0.5
    first = lax.broadcasted_iota(jnp.int32, (1, width), 1) < half

    mark = (
        lax.broadcasted_iota(jnp.int32, (width, 128), 0) // half
        == lax.broadcasted_iota(jnp.int32, (width, 128), 1) // 64
    ).astype(BF16)

    def top_norm(ref):
        x = ref[...]
        return jnp.max(
            jnp.dot(x * x, mark, preferred_element_type=F32), axis=0, keepdims=True
        )

    bound = jnp.max(top_norm(q_ref) * top_norm(k_ref))
    small = bound < (70.0 / scale) ** 2

    def finish(base, rows, mix, values):
        raw = jnp.dot(mix, values, preferred_element_type=F32)
        square = jnp.mean(raw * raw, axis=-1, keepdims=True)
        normed = raw * lax.rsqrt(square + EPSILON_NORM) * gain_ref[...]
        h_ref[pl.ds(base, rows), :] = normed.astype(BF16)

    @pl.when(small)
    def _():
        keep = lax.broadcasted_iota(jnp.int32, (bq, bq), 1) <= lax.broadcasted_iota(
            jnp.int32, (bq, bq), 0
        )
        keep_both = jnp.concatenate([keep, keep], axis=0)
        for i in range(seq // bq):
            slot = i % 2
            q = q_ref[i * bq : (i + 1) * bq, :]
            zero = jnp.zeros_like(q)
            both = jnp.concatenate(
                [jnp.where(first, q, zero), jnp.where(first, zero, q)], axis=0
            )
            for t in range(i + 1):
                scores = lax.dot_general(
                    both, k_ref[t * bq : (t + 1) * bq, :], NT, preferred_element_type=F32
                )
                e = jnp.exp2(scores * (scale * LOG2E))
                if t == i:
                    e = jnp.where(keep_both, e, 0.0)
                e_ref[slot, :, t * bq : (t + 1) * bq] = e
                part = e[:, :128]
                for c in range(1, bq // 128):
                    part = part + e[:, c * 128 : (c + 1) * 128]
                if t == 0:
                    sum_ref[slot] = part
                else:
                    sum_ref[slot] += part
            total = jnp.sum(sum_ref[slot], axis=-1, keepdims=True)
            one = 1.0 / total[:bq]
            two = lam / total[bq:]
            n = (i + 1) * bq
            mix = e_ref[slot, :bq, :n] * one - e_ref[slot, bq:, :n] * two
            finish(i * bq, bq, mix.astype(BF16), v_ref[:n, :])

    @pl.when(jnp.logical_not(small))
    def _():
        few = min(64, bq)

        def block(i, carry):
            base = pl.multiple_of(i * few, few)
            q = q_ref[pl.ds(base, few), :]
            zero = jnp.zeros_like(q)
            both = jnp.concatenate(
                [jnp.where(first, q, zero), jnp.where(first, zero, q)], axis=0
            )
            scores = (
                lax.dot_general(both, k_ref[...], NT, preferred_element_type=F32) * scale
            )
            row = lax.broadcasted_iota(jnp.int32, (few, seq), 0)
            keep = lax.broadcasted_iota(jnp.int32, (few, seq), 1) <= base + row
            scores = jnp.where(jnp.concatenate([keep, keep], axis=0), scores, -jnp.inf)
            e_ref[0, : 2 * few, :] = jnp.exp(
                scores - jnp.max(scores, axis=-1, keepdims=True)
            )
            total = jnp.sum(e_ref[0, : 2 * few, :], axis=-1, keepdims=True)
            mix = e_ref[0, :few, :] * (1.0 / total[:few]) - e_ref[0, few : 2 * few, :] * (
                lam / total[few:]
            )
            finish(base, few, mix.astype(BF16), v_ref[...])
            return carry

        lax.fori_loop(0, seq // few, block, 0)

    @pl.when(step == 0)
    def _():
        for copy in late_copies():
            copy.wait()

    h = h_ref[...]
    proj_ref[...] = jnp.dot(high_ref[...], h, preferred_element_type=F32) + jnp.dot(
        low_ref[...], h, preferred_element_type=F32
    )


def attend_heads(start, stop, query_rows, key_rows, value_rows, mix_lambda, head_gain, pairs, prev):
    seq = query_rows.shape[0]
    heads = mix_lambda.shape[0]
    count = stop - start
    width = query_rows.shape[1] // heads
    rank = pairs[0][0].shape[0]
    bq = min(256, seq)
    hbm = pl.BlockSpec(memory_space=pl.ANY)
    earlier = () if prev is None else (prev,)
    return pl.pallas_call(
        functools.partial(attend_kernel, bq, start),
        grid=(count,),
        out_shape=jax.ShapeDtypeStruct((rank, heads * DV), F32),
        in_specs=[
            pl.BlockSpec(memory_space=pltpu.SMEM),
            pl.BlockSpec(memory_space=pltpu.VMEM),
        ]
        + [hbm] * (7 + len(earlier)),
        out_specs=pl.BlockSpec((rank, DV), lambda j: (0, j + start)),
        input_output_aliases={9: 0} if earlier else {},
        scratch_shapes=[
            pltpu.VMEM((count, seq, width), BF16),
            pltpu.VMEM((count, seq, width), BF16),
            pltpu.VMEM((count, seq, DV), BF16),
            pltpu.VMEM((rank, seq), BF16),
            pltpu.VMEM((rank, seq), BF16),
            pltpu.VMEM((2, 2 * bq, seq), F32),
            pltpu.VMEM((seq, DV), BF16),
            pltpu.VMEM((2, 2 * bq, 128), F32),
            pltpu.SemaphoreType.DMA((count, 3)),
            pltpu.SemaphoreType.DMA((4,)),
        ],
        cost_estimate=pl.CostEstimate(
            flops=8 * count * seq * seq * DV,
            bytes_accessed=2 * seq * (count * (2 * width + DV) + 2 * rank),
            transcendentals=count * seq * seq,
        ),
        compiler_params=pltpu.CompilerParams(vmem_limit_bytes=VMEM_BYTES),
        name="attend_heads",
    )(
        mix_lambda,
        head_gain.reshape(1, DV),
        query_rows,
        key_rows,
        value_rows,
        *pairs[0],
        *pairs[1],
        *earlier,
    )


def out_final_kernel(entries, owner_ref, sum_ref, rank_owner_ref, basis_ref, *refs):
    parts, refs = refs[:4], refs[4:]
    direction, (copy_ref, step_ref, weight_ref, dir_ref, total_ref, held_ref, sems) = (
        refs[:-7], refs[-7:],
    )
    half, rows, share = parts[0].shape
    copies = []
    for p, part in enumerate(parts):
        copy = pltpu.make_async_copy(part, held_ref.at[pl.ds(p * half, half)], sems.at[p])
        copy.start()
        copies.append(copy)
    place_rows(rank_owner_ref, direction, dir_ref)
    high, low = split_pair(dir_ref[...].T)
    total_ref[...] = clip_of(sum_ref, entries) * (
        lax.dot_general(high, basis_ref[...], NT, preferred_element_type=F32)
        + lax.dot_general(low, basis_ref[...], NT, preferred_element_type=F32)
    )
    for p, copy in enumerate(copies):
        copy.wait()
        at = pl.ds((p // 2) * rows, rows)

        def one(a, carry):
            slot = p * half + a
            columns = pl.ds(pl.multiple_of(owner_ref[slot] * share, share), share)
            weight = held_ref[slot] - LEARN_RATE * total_ref[at, columns]
            copy_ref[at, columns] = weight.astype(BF16)
            return carry

        lax.fori_loop(0, half, one, 0)
    own = pl.ds(pl.multiple_of(owner_ref[0] * share, share), share)
    for g in range(2):
        at = pl.ds(g * rows, rows)
        step = total_ref[at, own]
        step_ref[at, :] = step
        weight_ref[at, :] = held_ref[2 * g * half] - LEARN_RATE * step


def out_final(owners, squares, entries, rank_owners, direction, basis, parts):
    half, rows, share = parts[0].shape
    width, rank = basis.shape
    cols = 2 * rows
    smem = pl.BlockSpec(memory_space=pltpu.SMEM)
    vmem = pl.BlockSpec(memory_space=pltpu.VMEM)
    block = jax.ShapeDtypeStruct((cols, share), F32)
    return pl.pallas_call(
        functools.partial(out_final_kernel, entries),
        out_shape=(jax.ShapeDtypeStruct((cols, width), BF16), block, block),
        in_specs=[smem, vmem, smem, vmem]
        + [pl.BlockSpec(memory_space=pl.ANY)] * 4
        + [vmem] * len(direction),
        out_specs=[vmem] * 3,
        scratch_shapes=[
            pltpu.VMEM((rank, cols), F32),
            pltpu.VMEM((cols, width), F32),
            pltpu.VMEM((4 * half, rows, share), F32),
            pltpu.SemaphoreType.DMA((4,)),
        ],
        cost_estimate=pl.CostEstimate(
            flops=4 * rank * cols * width,
            bytes_accessed=6 * cols * width,
            transcendentals=0,
        ),
        compiler_params=pltpu.CompilerParams(vmem_limit_bytes=VMEM_BYTES),
        name="out_final",
    )(owners, squares, rank_owners, basis, *parts, *direction)


def place_rows(owner_ref, parts, out_ref):
    blocks = owner_ref.shape[0] // len(parts)
    rows = parts[0].shape[0] // blocks
    for p, part in enumerate(parts):
        for a in range(blocks):
            at = pl.multiple_of(owner_ref[p * blocks + a] * rows, rows)
            out_ref[pl.ds(at, rows), :] = part[a * rows : (a + 1) * rows, :]


def clip_of(total_ref, entries):
    total = jnp.sum(
        jnp.sum(total_ref[...], axis=0, keepdims=True), axis=1, keepdims=True
    )
    return jnp.minimum(1.0, CLIP_RMS * math.sqrt(entries) / jnp.sqrt(total))


def value_final_kernel(
    entries, me_ref, sum_ref, owner_ref, basis_ref, old_ref, *refs
):
    parts, (step_ref, weight_ref, copy_ref, dir_ref) = refs[:-4], refs[-4:]
    place_rows(owner_ref, parts, dir_ref)
    high, low = split_pair(dir_ref[...])
    total = jnp.dot(basis_ref[...], high, preferred_element_type=F32) + jnp.dot(
        basis_ref[...], low, preferred_element_type=F32
    )
    step = clip_of(sum_ref, entries) * total
    weight = old_ref[...] - LEARN_RATE * step
    step_ref[...] = step
    weight_ref[...] = weight
    copy_ref[...] = weight.astype(BF16)


def value_final(me, squares, entries, owners, direction, basis, old):
    rows, cols = old.shape
    rank = basis.shape[1]
    block = jax.ShapeDtypeStruct((rows, cols), F32)
    whole = lambda shape: pl.BlockSpec(shape, lambda i, me: (0, 0))
    smem = pl.BlockSpec(memory_space=pltpu.SMEM)
    grid_spec = pltpu.PrefetchScalarGridSpec(
        num_scalar_prefetch=1,
        grid=(1,),
        in_specs=[
            whole(squares.shape),
            smem,
            pl.BlockSpec((rows, rank), lambda i, me: (me[0], 0)),
            whole((rows, cols)),
        ]
        + [whole(part.shape) for part in direction],
        out_specs=[whole((rows, cols))] * 3,
        scratch_shapes=[pltpu.VMEM((rank, cols), F32)],
    )
    return pl.pallas_call(
        functools.partial(value_final_kernel, entries),
        grid_spec=grid_spec,
        out_shape=(block, block, jax.ShapeDtypeStruct((rows, cols), BF16)),
        cost_estimate=pl.CostEstimate(
            flops=4 * rank * cols * rows,
            bytes_accessed=14 * old.size,
            transcendentals=0,
        ),
        name="value_final",
    )(me.reshape(1), squares, owners, basis, old, *direction)


def fold(part, arrived, inner, width, outer, groups, rows):
    cols = part.shape[1]
    vmem = pl.BlockSpec(memory_space=pltpu.VMEM)
    place = jnp.stack([inner, jnp.int32(width), outer]).astype(jnp.int32)
    return pl.pallas_call(
        functools.partial(fold_kernel, len(arrived)),
        out_shape=[jax.ShapeDtypeStruct((rows, cols), F32)] * groups,
        in_specs=[pl.BlockSpec(memory_space=pltpu.SMEM)] + [vmem] * (1 + len(arrived)),
        out_specs=[vmem] * groups,
        cost_estimate=pl.CostEstimate(
            flops=part.size, bytes_accessed=8 * part.size, transcendentals=0
        ),
        name="fold",
    )(place, part, *arrived)


def fold_kernel(count, place_ref, part_ref, *refs):
    arrived, outs = refs[:count], refs[count:]
    rows = outs[0].shape[0]
    for d, out in enumerate(outs):
        member = place_ref[2] ^ d
        at = pl.multiple_of((member * place_ref[1] + place_ref[0]) * rows, rows)
        total = part_ref[pl.ds(at, rows), :]
        for other in arrived:
            total = total + other[pl.ds(pl.multiple_of(member * rows, rows), rows), :]
        out[...] = total


def square_kernel(*refs):
    parts, out_ref = refs[:-1], refs[-1]
    sums = []
    for part in parts:
        rows, cols = part.shape
        total = jnp.zeros((8, 128), F32)
        for r in range(rows // 8):
            for c in range(cols // 128):
                x = part[r * 8 : (r + 1) * 8, c * 128 : (c + 1) * 128]
                total = total + x * x
        sums.append(total)
    while len(sums) > 1:
        sums = [a + b for a, b in zip(sums[::2], sums[1::2])]
    out_ref[...] = sums[0]


def square_sums(parts):
    vmem = pl.BlockSpec(memory_space=pltpu.VMEM)
    return pl.pallas_call(
        square_kernel,
        out_shape=jax.ShapeDtypeStruct((8, 128), F32),
        in_specs=[vmem] * len(parts),
        out_specs=vmem,
        cost_estimate=pl.CostEstimate(
            flops=2 * len(parts) * parts[0].size,
            bytes_accessed=4 * len(parts) * parts[0].size,
            transcendentals=0,
        ),
        name="square_sums",
    )(*parts)


def assemble_kernel(owner_ref, *refs):
    parts, out_ref = refs[:4], refs[4]
    half, rows, _ = parts[0].shape
    for p, part in enumerate(parts):
        def one(a, carry):
            at = pl.multiple_of(owner_ref[p * half + a] * (2 * rows) + (p // 2) * rows, rows)
            out_ref[pl.ds(at, rows), :] = part[a]
            return carry

        lax.fori_loop(0, half, one, 0)


def assemble(owners, parts):
    half, rows, cols = parts[0].shape
    vmem = pl.BlockSpec(memory_space=pltpu.VMEM)
    return pl.pallas_call(
        assemble_kernel,
        out_shape=jax.ShapeDtypeStruct((4 * half * rows, cols), parts[0].dtype),
        in_specs=[pl.BlockSpec(memory_space=pltpu.SMEM)] + [vmem] * 4,
        out_specs=vmem,
        cost_estimate=pl.CostEstimate(
            flops=0, bytes_accessed=16 * half * rows * cols, transcendentals=0
        ),
        compiler_params=pltpu.CompilerParams(vmem_limit_bytes=VMEM_BYTES),
        name="assemble",
    )(owners, *parts)


def swap(x, axis, bit):
    n = lax.axis_size(axis)
    return lax.ppermute(x, axis, [(i, i ^ bit) for i in range(n)])


def bits_down(n):
    bits = [1 << b for b in range(n.bit_length() - 1)]
    return bits[::-1]


def groups_of(axis):
    n = lax.axis_size(axis)
    outer = min(4, n)
    return outer, n // outer


def reduce_scatter(x, axis):
    outer, inner = groups_of(axis)
    me = lax.axis_index(axis)
    rows, cols = x.shape[0] // (outer * inner), x.shape[1]
    place_out, place_in = me // inner, me % inner
    blocks = x.reshape(outer, inner, rows, cols)
    arrived = []
    for d in range(1, inner):
        send = lax.dynamic_index_in_dim(blocks, place_in ^ d, 1, keepdims=False)
        arrived.append(swap(send.reshape(outer * rows, cols), axis, d))
    sums = fold(x, arrived, place_in, inner, place_out, outer, rows)
    total = sums[0]
    for d in range(1, outer):
        total = total + swap(sums[d], axis, d * inner)
    return total


def gather_and_square(x):
    axis = "fs"
    outer, inner = groups_of(axis)
    near = [x] + [swap(x, axis, d * inner) for d in range(1, outer)]
    squares = square_sums(near)
    near = jnp.concatenate(near, axis=0)
    parts = [near] + [swap(near, axis, d) for d in range(1, inner)]
    away = [p ^ (d * inner) for p in range(inner) for d in range(outer)]
    owners = jnp.array(away, jnp.int32) ^ lax.axis_index(axis)
    squares = sum_over(squares, "tp", lax.axis_size("tp"))
    squares = sum_over(squares, axis, inner)
    return parts, owners, squares, x.size * lax.axis_size(axis) * lax.axis_size("tp")


def gather_by_distance(x, axis):
    bits = bits_down(lax.axis_size(axis))
    other = swap(x, axis, bits[0])
    rows = x.shape[0] // 2
    parts, owners = [], []
    for g, order in enumerate((bits[:0:-1], bits[1:])):
        cut = slice(g * rows, (g + 1) * rows)
        piece = jnp.stack([x[cut], other[cut]])
        away = [0, bits[0]]
        for bit in order[:-1]:
            piece = jnp.concatenate([piece, swap(piece, axis, bit)])
            away = away + [a ^ bit for a in away]
        last = order[-1]
        parts += [piece, swap(piece, axis, last)]
        owners += away + [a ^ last for a in away]
    return parts, jnp.array(owners, jnp.int32) ^ lax.axis_index(axis)


def sum_over(x, axis, group):
    for bit in bits_down(group)[::-1]:
        x = x + swap(x, axis, bit)
    return x


def moment_step(proj, first, second):
    new_first = BETA_ONE * first + (1.0 - BETA_ONE) * proj
    new_second = BETA_TWO * second + (1.0 - BETA_TWO) * proj * proj
    direction = new_first / (jnp.sqrt(new_second) + EPSILON_ADAM)
    return (new_first, new_second, direction)


def body(
    query_rows,
    key_rows,
    value_rows,
    mix_lambda,
    head_gain,
    out_cotangent,
    layer_input,
    value_cotangent,
    out_weight,
    value_weight,
    out_basis,
    value_basis,
    out_first,
    out_second,
    value_first,
    value_second,
):
    me = lax.axis_index("fs")
    parts, owners = gather_by_distance(out_weight, "fs")

    value_part = value_proj(layer_input, value_cotangent, value_basis)
    value_sum = reduce_scatter(value_part, "fs")
    new_value_first, new_value_second, value_dir = moment_step(
        value_sum, value_first, value_second
    )
    value_dirs, value_owners, *value_squares = gather_and_square(value_dir)
    value_step, new_value_weight, value_rounded = value_final(
        me, *value_squares, value_owners, value_dirs, value_basis, value_weight
    )
    value_copy = assemble(owners, gather_by_distance(value_rounded, "fs")[0])

    pairs = [low_rank_rows(half, out_cotangent, out_basis) for half in range(2)]
    heads = mix_lambda.shape[0]
    out_part = None
    cuts = sorted({0, heads // 4, heads // 2, heads})
    for start, stop in zip(cuts[:-1], cuts[1:]):
        out_part = attend_heads(
            start, stop, query_rows, key_rows,
            value_rows, mix_lambda, head_gain, pairs, out_part,
        )
    out_sum = reduce_scatter(out_part, "fs")
    new_out_first, new_out_second, out_dir = moment_step(out_sum, out_first, out_second)
    out_dirs, out_owners, *out_squares = gather_and_square(out_dir)
    out_copy, out_step, new_out_weight = out_final(
        owners, *out_squares, out_owners, out_dirs, out_basis, parts
    )
    return (
        out_step,
        value_step,
        new_out_weight,
        new_value_weight,
        out_copy,
        value_copy,
        new_out_first,
        new_out_second,
        new_value_first,
        new_value_second,
    )


def solution(mesh):
    split, rows = P("fs", "tp"), P("fs", None)
    placed = (
        split, split, split, P("tp"), P(), rows, rows, split,
        P("tp", "fs"), split, P(), P(), split, split, split, split,
    )
    return jax.shard_map(
        body,
        mesh=mesh,
        in_specs=placed,
        out_specs=(
            P("tp", "fs"), split, P("tp", "fs"), split, P("tp", None), P(None, "tp"),
            split, split, split, split,
        ),
        check_vma=False,
    )
```

```python
import functools
import math

import jax
import jax.numpy as jnp
from jax import lax
from jax.experimental import pallas as pl
from jax.experimental.pallas import tpu as pltpu
from jax.sharding import PartitionSpec as P

DV = 128

EPSILON_NORM = 1e-05
EPSILON_ADAM = 1e-08
BETA_ONE = 0.9
BETA_TWO = 0.95
CLIP_RMS = 1.0
LEARN_RATE = 0.01
LOG2E = math.log2(math.e)

F32 = jnp.float32
BF16 = jnp.bfloat16
NT = (((1,), (1,)), ((), ()))
VMEM_BYTES = 60 * 2**20


def split_pair(x):
    high = x.astype(BF16)
    return high, (x - high.astype(F32)).astype(BF16)


def write_sends(place_ref, outer, proj_ref, send_refs):
    inner = len(send_refs) + 1
    rows = proj_ref.shape[0] // (outer * inner)
    for d, send_ref in enumerate(send_refs, 1):
        member = place_ref[0] ^ d
        for p in range(outer):
            at = pl.multiple_of((p * inner + member) * rows, rows)
            send_ref[p * rows : (p + 1) * rows, :] = proj_ref[pl.ds(at, rows), :]


def value_proj_kernel(outer, place_ref, x_ref, c_ref, basis_ref, proj_ref, *send_refs):
    y = jnp.dot(x_ref[...], basis_ref[...], preferred_element_type=F32)
    high, low = split_pair(y.T)
    part = jnp.dot(high, c_ref[...], preferred_element_type=F32) + jnp.dot(
        low, c_ref[...], preferred_element_type=F32
    )

    @pl.when(pl.program_id(0) == 0)
    def _():
        proj_ref[...] = part

    @pl.when(pl.program_id(0) > 0)
    def _():
        proj_ref[...] += part


    @pl.when(pl.program_id(0) == pl.num_programs(0) - 1)
    def _():
        write_sends(place_ref, outer, proj_ref, send_refs)


def sends_shape(rank, cols):
    _, inner = groups_of("fs")
    return [jax.ShapeDtypeStruct((rank // inner, cols), F32)] * (inner - 1)


def value_proj(place, x, c, basis):
    tokens, width = x.shape
    rank, cols = basis.shape[1], c.shape[1]
    block = min(512, tokens)
    outer, inner = groups_of("fs")
    return pl.pallas_call(
        functools.partial(value_proj_kernel, outer),
        grid=(tokens // block,),
        out_shape=[jax.ShapeDtypeStruct((rank, cols), F32)] + sends_shape(rank, cols),
        in_specs=[
            pl.BlockSpec(memory_space=pltpu.SMEM),
            pl.BlockSpec((block, width), lambda t: (t, 0)),
            pl.BlockSpec((block, cols), lambda t: (t, 0)),
            pl.BlockSpec((width, rank), lambda t: (0, 0)),
        ],
        out_specs=[pl.BlockSpec((rank, cols), lambda t: (0, 0))]
        + [pl.BlockSpec((rank // inner, cols), lambda t: (0, 0))] * (inner - 1),
        cost_estimate=pl.CostEstimate(
            flops=2 * tokens * rank * (width + 2 * cols),
            bytes_accessed=2 * tokens * (width + cols),
            transcendentals=0,
        ),
        compiler_params=pltpu.CompilerParams(vmem_limit_bytes=VMEM_BYTES),
        name="value_proj",
    )(place, x, c, basis)


def low_rank_kernel(x_ref, basis_ref, high_ref, low_ref):
    y = jnp.dot(x_ref[...], basis_ref[...], preferred_element_type=F32)
    high_ref[...], low_ref[...] = split_pair(y)


def low_rank_rows(half, x, basis):
    tokens, width = x.shape[0] // 2, x.shape[1]
    rank = basis.shape[1]
    block = min(512, tokens)
    skip = half * (tokens // block)
    out = jax.ShapeDtypeStruct((tokens, rank), BF16)
    return pl.pallas_call(
        low_rank_kernel,
        grid=(tokens // block,),
        out_shape=(out, out),
        in_specs=[
            pl.BlockSpec((block, width), lambda t: (t + skip, 0)),
            pl.BlockSpec((width, rank), lambda t: (0, 0)),
        ],
        out_specs=[pl.BlockSpec((block, rank), lambda t: (t, 0))] * 2,
        cost_estimate=pl.CostEstimate(
            flops=2 * tokens * rank * width,
            bytes_accessed=2 * tokens * width,
            transcendentals=0,
        ),
        compiler_params=pltpu.CompilerParams(vmem_limit_bytes=VMEM_BYTES),
        name="low_rank_rows",
    )(x, basis)


def attend_kernel(
    bq, start, outer, inner, place_ref, lam_ref, gain_ref, q_hbm, k_hbm, v_hbm, high_hbm,
    low_hbm, high_two, low_two, *rest
):
    q_all, k_all, v_all, high_ref, low_ref, e_ref, h_ref, sum_ref, sems, late_sems = rest[-10:]
    proj_ref, *send_refs = rest[-10 - inner : -10]
    count, seq, width = q_all.shape
    step = pl.program_id(0)

    def head_copies(j):
        columns = pl.ds(pl.multiple_of((start + j) * width, width), width)
        return [
            pltpu.make_async_copy(source.at[:, columns], target.at[j], sems.at[j, i])
            for i, (source, target) in enumerate(
                ((k_hbm, k_all), (q_hbm, q_all), (v_hbm, v_all))
            )
        ]

    def late_copies():
        pairs = ((high_hbm, high_ref), (low_hbm, low_ref), (high_two, high_ref), (low_two, low_ref))
        return [
            pltpu.make_async_copy(
                source,
                target.at[pl.ds(i // 2 * (seq // 2), seq // 2), :],
                late_sems.at[i],
            )
            for i, (source, target) in enumerate(pairs)
        ]

    @pl.when(step == 0)
    def _():
        for copy in head_copies(0):
            copy.start()

    for copy in head_copies(step):
        copy.wait()

    @pl.when(step == 0)
    def _():
        for copy in late_copies():
            copy.start()
        for j in range(1, count):
            for copy in head_copies(j):
                copy.start()

    q_ref, k_ref, v_ref = q_all.at[step], k_all.at[step], v_all.at[step]
    half = width // 2
    lam = lam_ref[start + step]
    scale = half**-0.5
    first = lax.broadcasted_iota(jnp.int32, (1, width), 1) < half

    def finish(base, rows, mix, values):
        raw = jnp.dot(mix, values, preferred_element_type=F32)
        square = jnp.mean(raw * raw, axis=-1, keepdims=True)
        normed = raw * lax.rsqrt(square + EPSILON_NORM) * gain_ref[...]
        h_ref[:, pl.ds(base, rows)] = normed.T.astype(BF16)

    keep = lax.broadcasted_iota(jnp.int32, (bq, bq), 1) <= lax.broadcasted_iota(
        jnp.int32, (bq, bq), 0
    )
    keep_both = jnp.concatenate([keep, keep], axis=0)
    for i in range(seq // bq):
        slot = i % 2
        q = q_ref[i * bq : (i + 1) * bq, :]
        zero = jnp.zeros_like(q)
        both = jnp.concatenate(
            [jnp.where(first, q, zero), jnp.where(first, zero, q)], axis=0
        )
        for t in range(i + 1):
            scores = lax.dot_general(
                both, k_ref[t * bq : (t + 1) * bq, :], NT, preferred_element_type=F32
            )
            e = jnp.exp2(scores * (scale * LOG2E))
            if t == i:
                e = jnp.where(keep_both, e, 0.0)
            e_ref[slot, :, t * bq : (t + 1) * bq] = e
            part = e[:, :128]
            for c in range(1, bq // 128):
                part = part + e[:, c * 128 : (c + 1) * 128]
            if t == 0:
                sum_ref[slot] = part
            else:
                sum_ref[slot] += part
        total = jnp.sum(sum_ref[slot], axis=-1, keepdims=True)
        most = total if i == 0 else jnp.maximum(most, total)
        least = total if i == 0 else jnp.minimum(least, total)
        one = 1.0 / total[:bq]
        two = lam / total[bq:]
        n = (i + 1) * bq
        mix = e_ref[slot, :bq, :n] * one - e_ref[slot, bq:, :n] * two
        finish(i * bq, bq, mix.astype(BF16), v_ref[:n, :])
    fine = (jnp.max(most) < 2.0**120) & (jnp.min(least) > 2.0**-60)

    @pl.when(jnp.logical_not(fine))
    def _():
        few = min(128, bq)

        def block(i, carry):
            base = pl.multiple_of(i * few, few)
            q = q_ref[pl.ds(base, few), :]
            zero = jnp.zeros_like(q)
            both = jnp.concatenate(
                [jnp.where(first, q, zero), jnp.where(first, zero, q)], axis=0
            )
            scores = (
                lax.dot_general(both, k_ref[...], NT, preferred_element_type=F32) * scale
            )
            row = lax.broadcasted_iota(jnp.int32, (few, seq), 0)
            keep = lax.broadcasted_iota(jnp.int32, (few, seq), 1) <= base + row
            scores = jnp.where(jnp.concatenate([keep, keep], axis=0), scores, -jnp.inf)
            e_ref[0, : 2 * few, :] = jnp.exp(
                scores - jnp.max(scores, axis=-1, keepdims=True)
            )
            total = jnp.sum(e_ref[0, : 2 * few, :], axis=-1, keepdims=True)
            mix = e_ref[0, :few, :] * (1.0 / total[:few]) - e_ref[0, few : 2 * few, :] * (
                lam / total[few:]
            )
            finish(base, few, mix.astype(BF16), v_ref[...])
            return carry

        lax.fori_loop(0, seq // few, block, 0)

    @pl.when(step == 0)
    def _():
        for copy in late_copies():
            copy.wait()

    h = h_ref[...]
    turned = jnp.dot(h, high_ref[...], preferred_element_type=F32) + jnp.dot(
        h, low_ref[...], preferred_element_type=F32
    )
    proj_ref[...] = turned.T
    write_sends(place_ref, outer, proj_ref, send_refs)


def attend_heads(
    start, stop, place, query_rows, key_rows, value_rows, mix_lambda, head_gain, pairs,
    earlier,
):
    seq = query_rows.shape[0]
    heads = mix_lambda.shape[0]
    count = stop - start
    width = query_rows.shape[1] // heads
    rank = pairs[0][0].shape[1]
    bq = min(256, seq)
    outer, inner = groups_of("fs")
    hbm = pl.BlockSpec(memory_space=pl.ANY)
    return pl.pallas_call(
        functools.partial(attend_kernel, bq, start, outer, inner),
        grid=(count,),
        out_shape=[jax.ShapeDtypeStruct((rank, heads * DV), F32)]
        + sends_shape(rank, heads * DV),
        in_specs=[
            pl.BlockSpec(memory_space=pltpu.SMEM),
            pl.BlockSpec(memory_space=pltpu.SMEM),
            pl.BlockSpec(memory_space=pltpu.VMEM),
        ]
        + [hbm] * (7 + len(earlier)),
        out_specs=[pl.BlockSpec((rank, DV), lambda j: (0, j + start))]
        + [pl.BlockSpec((rank // inner, DV), lambda j: (0, j + start))] * (inner - 1),
        input_output_aliases={10 + i: i for i in range(len(earlier))},
        scratch_shapes=[
            pltpu.VMEM((count, seq, width), BF16),
            pltpu.VMEM((count, seq, width), BF16),
            pltpu.VMEM((count, seq, DV), BF16),
            pltpu.VMEM((seq, rank), BF16),
            pltpu.VMEM((seq, rank), BF16),
            pltpu.VMEM((2, 2 * bq, seq), F32),
            pltpu.VMEM((DV, seq), BF16),
            pltpu.VMEM((2, 2 * bq, 128), F32),
            pltpu.SemaphoreType.DMA((count, 3)),
            pltpu.SemaphoreType.DMA((4,)),
        ],
        cost_estimate=pl.CostEstimate(
            flops=8 * count * seq * seq * DV,
            bytes_accessed=2 * seq * (count * (2 * width + DV) + 2 * rank),
            transcendentals=count * seq * seq,
        ),
        compiler_params=pltpu.CompilerParams(vmem_limit_bytes=VMEM_BYTES),
        name="attend_heads",
    )(
        place,
        mix_lambda,
        head_gain.reshape(1, DV),
        query_rows,
        key_rows,
        value_rows,
        *pairs[0],
        *pairs[1],
        *earlier,
    )


def out_final_kernel(entries, owner_ref, sum_ref, rank_owner_ref, basis_ref, *refs):
    parts, refs = refs[:4], refs[4:]
    direction, (copy_ref, step_ref, weight_ref, dir_ref, total_ref, held_ref, sems) = (
        refs[:-7], refs[-7:],
    )
    half, rows, share = parts[0].shape
    copies = []
    for p, part in enumerate(parts):
        copy = pltpu.make_async_copy(part, held_ref.at[pl.ds(p * half, half)], sems.at[p])
        copy.start()
        copies.append(copy)
    place_rows(rank_owner_ref, direction, dir_ref)
    high, low = split_pair(dir_ref[...].T)
    total_ref[...] = clip_of(sum_ref, entries) * (
        lax.dot_general(high, basis_ref[...], NT, preferred_element_type=F32)
        + lax.dot_general(low, basis_ref[...], NT, preferred_element_type=F32)
    )
    for p, copy in enumerate(copies):
        copy.wait()
        at = pl.ds((p // 2) * rows, rows)

        def one(a, carry):
            slot = p * half + a
            columns = pl.ds(pl.multiple_of(owner_ref[slot] * share, share), share)
            weight = held_ref[slot] - LEARN_RATE * total_ref[at, columns]
            copy_ref[at, columns] = weight.astype(BF16)
            return carry

        lax.fori_loop(0, half, one, 0)
    own = pl.ds(pl.multiple_of(owner_ref[0] * share, share), share)
    for g in range(2):
        at = pl.ds(g * rows, rows)
        step = total_ref[at, own]
        step_ref[at, :] = step
        weight_ref[at, :] = held_ref[2 * g * half] - LEARN_RATE * step


def out_final(owners, squares, entries, rank_owners, direction, basis, parts):
    half, rows, share = parts[0].shape
    width, rank = basis.shape
    cols = 2 * rows
    smem = pl.BlockSpec(memory_space=pltpu.SMEM)
    vmem = pl.BlockSpec(memory_space=pltpu.VMEM)
    block = jax.ShapeDtypeStruct((cols, share), F32)
    return pl.pallas_call(
        functools.partial(out_final_kernel, entries),
        out_shape=(jax.ShapeDtypeStruct((cols, width), BF16), block, block),
        in_specs=[smem, vmem, smem, vmem]
        + [pl.BlockSpec(memory_space=pl.ANY)] * 4
        + [vmem] * len(direction),
        out_specs=[vmem] * 3,
        scratch_shapes=[
            pltpu.VMEM((rank, cols), F32),
            pltpu.VMEM((cols, width), F32),
            pltpu.VMEM((4 * half, rows, share), F32),
            pltpu.SemaphoreType.DMA((4,)),
        ],
        cost_estimate=pl.CostEstimate(
            flops=4 * rank * cols * width,
            bytes_accessed=6 * cols * width,
            transcendentals=0,
        ),
        compiler_params=pltpu.CompilerParams(vmem_limit_bytes=VMEM_BYTES),
        name="out_final",
    )(owners, squares, rank_owners, basis, *parts, *direction)


def place_rows(owner_ref, parts, out_ref):
    blocks = owner_ref.shape[0] // len(parts)
    rows = parts[0].shape[0] // blocks
    for p, part in enumerate(parts):
        for a in range(blocks):
            at = pl.multiple_of(owner_ref[p * blocks + a] * rows, rows)
            out_ref[pl.ds(at, rows), :] = part[a * rows : (a + 1) * rows, :]


def clip_of(total_ref, entries):
    total = jnp.sum(
        jnp.sum(total_ref[...], axis=0, keepdims=True), axis=1, keepdims=True
    )
    return jnp.minimum(1.0, CLIP_RMS * math.sqrt(entries) / jnp.sqrt(total))


def value_final_kernel(
    entries, me_ref, sum_ref, owner_ref, basis_ref, old_ref, *refs
):
    parts, (step_ref, weight_ref, copy_ref, dir_ref) = refs[:-4], refs[-4:]
    place_rows(owner_ref, parts, dir_ref)
    high, low = split_pair(dir_ref[...])
    total = jnp.dot(basis_ref[...], high, preferred_element_type=F32) + jnp.dot(
        basis_ref[...], low, preferred_element_type=F32
    )
    step = clip_of(sum_ref, entries) * total
    weight = old_ref[...] - LEARN_RATE * step
    step_ref[...] = step
    weight_ref[...] = weight
    copy_ref[...] = weight.astype(BF16)


def value_final(me, squares, entries, owners, direction, basis, old):
    rows, cols = old.shape
    rank = basis.shape[1]
    block = jax.ShapeDtypeStruct((rows, cols), F32)
    whole = lambda shape: pl.BlockSpec(shape, lambda i, me: (0, 0))
    smem = pl.BlockSpec(memory_space=pltpu.SMEM)
    grid_spec = pltpu.PrefetchScalarGridSpec(
        num_scalar_prefetch=1,
        grid=(1,),
        in_specs=[
            whole(squares.shape),
            smem,
            pl.BlockSpec((rows, rank), lambda i, me: (me[0], 0)),
            whole((rows, cols)),
        ]
        + [whole(part.shape) for part in direction],
        out_specs=[whole((rows, cols))] * 3,
        scratch_shapes=[pltpu.VMEM((rank, cols), F32)],
    )
    return pl.pallas_call(
        functools.partial(value_final_kernel, entries),
        grid_spec=grid_spec,
        out_shape=(block, block, jax.ShapeDtypeStruct((rows, cols), BF16)),
        cost_estimate=pl.CostEstimate(
            flops=4 * rank * cols * rows,
            bytes_accessed=14 * old.size,
            transcendentals=0,
        ),
        name="value_final",
    )(me.reshape(1), squares, owners, basis, old, *direction)


def fold(part, arrived, inner, width, outer, groups, rows):
    cols = part.shape[1]
    vmem = pl.BlockSpec(memory_space=pltpu.VMEM)
    place = jnp.stack([inner, jnp.int32(width), outer]).astype(jnp.int32)
    return pl.pallas_call(
        functools.partial(fold_kernel, len(arrived)),
        out_shape=[jax.ShapeDtypeStruct((rows, cols), F32)] * groups,
        in_specs=[pl.BlockSpec(memory_space=pltpu.SMEM)] + [vmem] * (1 + len(arrived)),
        out_specs=[vmem] * groups,
        cost_estimate=pl.CostEstimate(
            flops=part.size, bytes_accessed=8 * part.size, transcendentals=0
        ),
        name="fold",
    )(place, part, *arrived)


def fold_kernel(count, place_ref, part_ref, *refs):
    arrived, outs = refs[:count], refs[count:]
    rows = outs[0].shape[0]
    for d, out in enumerate(outs):
        member = place_ref[2] ^ d
        at = pl.multiple_of((member * place_ref[1] + place_ref[0]) * rows, rows)
        total = part_ref[pl.ds(at, rows), :]
        for other in arrived:
            total = total + other[pl.ds(pl.multiple_of(member * rows, rows), rows), :]
        out[...] = total


def square_kernel(*refs):
    parts, out_ref = refs[:-1], refs[-1]
    sums = []
    for part in parts:
        rows, cols = part.shape
        total = jnp.zeros((8, 128), F32)
        for r in range(rows // 8):
            for c in range(cols // 128):
                x = part[r * 8 : (r + 1) * 8, c * 128 : (c + 1) * 128]
                total = total + x * x
        sums.append(total)
    while len(sums) > 1:
        sums = [a + b for a, b in zip(sums[::2], sums[1::2])]
    out_ref[...] = sums[0]


def square_sums(parts):
    vmem = pl.BlockSpec(memory_space=pltpu.VMEM)
    return pl.pallas_call(
        square_kernel,
        out_shape=jax.ShapeDtypeStruct((8, 128), F32),
        in_specs=[vmem] * len(parts),
        out_specs=vmem,
        cost_estimate=pl.CostEstimate(
            flops=2 * len(parts) * parts[0].size,
            bytes_accessed=4 * len(parts) * parts[0].size,
            transcendentals=0,
        ),
        name="square_sums",
    )(*parts)


def assemble_kernel(owner_ref, *refs):
    parts, out_ref = refs[:4], refs[4]
    half, rows, _ = parts[0].shape
    for p, part in enumerate(parts):
        def one(a, carry):
            at = pl.multiple_of(owner_ref[p * half + a] * (2 * rows) + (p // 2) * rows, rows)
            out_ref[pl.ds(at, rows), :] = part[a]
            return carry

        lax.fori_loop(0, half, one, 0)


def assemble(owners, parts):
    half, rows, cols = parts[0].shape
    vmem = pl.BlockSpec(memory_space=pltpu.VMEM)
    return pl.pallas_call(
        assemble_kernel,
        out_shape=jax.ShapeDtypeStruct((4 * half * rows, cols), parts[0].dtype),
        in_specs=[pl.BlockSpec(memory_space=pltpu.SMEM)] + [vmem] * 4,
        out_specs=vmem,
        cost_estimate=pl.CostEstimate(
            flops=0, bytes_accessed=16 * half * rows * cols, transcendentals=0
        ),
        compiler_params=pltpu.CompilerParams(vmem_limit_bytes=VMEM_BYTES),
        name="assemble",
    )(owners, *parts)


def swap(x, axis, bit):
    n = lax.axis_size(axis)
    return lax.ppermute(x, axis, [(i, i ^ bit) for i in range(n)])


def bits_down(n):
    bits = [1 << b for b in range(n.bit_length() - 1)]
    return bits[::-1]


def groups_of(axis):
    n = lax.axis_size(axis)
    outer = min(4, n)
    return outer, n // outer


def reduce_scatter(x, sends, axis):
    outer, inner = groups_of(axis)
    me = lax.axis_index(axis)
    rows = x.shape[0] // (outer * inner)
    arrived = [swap(send, axis, d) for d, send in enumerate(sends, 1)]
    sums = fold(x, arrived, me % inner, inner, me // inner, outer, rows)
    total = sums[0]
    for d in range(1, outer):
        total = total + swap(sums[d], axis, d * inner)
    return total


def gather_and_square(x):
    axis = "fs"
    outer, inner = groups_of(axis)
    near = [x] + [swap(x, axis, d * inner) for d in range(1, outer)]
    squares = square_sums(near)
    near = jnp.concatenate(near, axis=0)
    parts = [near] + [swap(near, axis, d) for d in range(1, inner)]
    away = [p ^ (d * inner) for p in range(inner) for d in range(outer)]
    owners = jnp.array(away, jnp.int32) ^ lax.axis_index(axis)
    squares = sum_over(squares, "tp", lax.axis_size("tp"))
    squares = sum_over(squares, axis, inner)
    return parts, owners, squares, x.size * lax.axis_size(axis) * lax.axis_size("tp")


def gather_by_distance(x, axis):
    bits = bits_down(lax.axis_size(axis))
    other = swap(x, axis, bits[0])
    rows = x.shape[0] // 2
    parts, owners = [], []
    for g, order in enumerate((bits[:0:-1], bits[1:])):
        cut = slice(g * rows, (g + 1) * rows)
        piece = jnp.stack([x[cut], other[cut]])
        away = [0, bits[0]]
        for bit in order[:-1]:
            piece = jnp.concatenate([piece, swap(piece, axis, bit)])
            away = away + [a ^ bit for a in away]
        last = order[-1]
        parts += [piece, swap(piece, axis, last)]
        owners += away + [a ^ last for a in away]
    return parts, jnp.array(owners, jnp.int32) ^ lax.axis_index(axis)


def sum_over(x, axis, group):
    for bit in bits_down(group)[::-1]:
        x = x + swap(x, axis, bit)
    return x


def moment_step(proj, first, second):
    new_first = BETA_ONE * first + (1.0 - BETA_ONE) * proj
    new_second = BETA_TWO * second + (1.0 - BETA_TWO) * proj * proj
    direction = new_first / (jnp.sqrt(new_second) + EPSILON_ADAM)
    return (new_first, new_second, direction)


def body(
    query_rows,
    key_rows,
    value_rows,
    mix_lambda,
    head_gain,
    out_cotangent,
    layer_input,
    value_cotangent,
    out_weight,
    value_weight,
    out_basis,
    value_basis,
    out_first,
    out_second,
    value_first,
    value_second,
):
    me = lax.axis_index("fs")
    parts, owners = gather_by_distance(out_weight, "fs")

    place = (me % groups_of("fs")[1]).reshape(1)
    value_part, *value_sends = value_proj(place, layer_input, value_cotangent, value_basis)
    value_sum = reduce_scatter(value_part, value_sends, "fs")
    new_value_first, new_value_second, value_dir = moment_step(
        value_sum, value_first, value_second
    )
    value_dirs, value_owners, *value_squares = gather_and_square(value_dir)
    value_step, new_value_weight, value_rounded = value_final(
        me, *value_squares, value_owners, value_dirs, value_basis, value_weight
    )
    value_copy = assemble(owners, gather_by_distance(value_rounded, "fs")[0])

    pairs = [low_rank_rows(half, out_cotangent, out_basis) for half in range(2)]
    heads = mix_lambda.shape[0]
    out_parts = ()
    cuts = sorted({0, heads // 4, heads // 2, heads})
    for start, stop in zip(cuts[:-1], cuts[1:]):
        out_parts = attend_heads(
            start, stop, place, query_rows, key_rows, value_rows, mix_lambda,
            head_gain, pairs, out_parts,
        )
    out_sum = reduce_scatter(out_parts[0], out_parts[1:], "fs")
    new_out_first, new_out_second, out_dir = moment_step(out_sum, out_first, out_second)
    out_dirs, out_owners, *out_squares = gather_and_square(out_dir)
    out_copy, out_step, new_out_weight = out_final(
        owners, *out_squares, out_owners, out_dirs, out_basis, parts
    )
    return (
        out_step,
        value_step,
        new_out_weight,
        new_value_weight,
        out_copy,
        value_copy,
        new_out_first,
        new_out_second,
        new_value_first,
        new_value_second,
    )


def solution(mesh):
    split, rows = P("fs", "tp"), P("fs", None)
    placed = (
        split, split, split, P("tp"), P(), rows, rows, split,
        P("tp", "fs"), split, P(), P(), split, split, split, split,
    )
    return jax.shard_map(
        body,
        mesh=mesh,
        in_specs=placed,
        out_specs=(
            P("tp", "fs"), split, P("tp", "fs"), split, P("tp", None), P(None, "tp"),
            split, split, split, split,
        ),
        check_vma=False,
    )
```

```python
import functools
import math

import jax
import jax.numpy as jnp
from jax import lax
from jax.experimental import pallas as pl
from jax.experimental.pallas import tpu as pltpu
from jax.sharding import PartitionSpec as P

DV = 128

EPSILON_NORM = 1e-05
EPSILON_ADAM = 1e-08
BETA_ONE = 0.9
BETA_TWO = 0.95
CLIP_RMS = 1.0
LEARN_RATE = 0.01
LOG2E = math.log2(math.e)

F32 = jnp.float32
BF16 = jnp.bfloat16
NT = (((1,), (1,)), ((), ()))
VMEM_BYTES = 60 * 2**20
KERNEL_BYTES = 24 * 2**20


def split_pair(x):
    high = x.astype(BF16)
    return high, (x - high.astype(F32)).astype(BF16)


def write_sends(place_ref, outer, proj_ref, send_refs):
    inner = len(send_refs) + 1
    rows = proj_ref.shape[0] // (outer * inner)
    for d, send_ref in enumerate(send_refs, 1):
        member = place_ref[0] ^ d
        for p in range(outer):
            at = pl.multiple_of((p * inner + member) * rows, rows)
            send_ref[p * rows : (p + 1) * rows, :] = proj_ref[pl.ds(at, rows), :]


def in_hbm(x):
    return pltpu.with_memory_space_constraint(x, pltpu.HBM)


def fetch(step, last, copies):
    @pl.when(step == 0)
    def _():
        for copy in copies():
            copy.start()

    def finish():
        @pl.when(step == last)
        def _():
            for copy in copies():
                copy.wait()

    return finish


def value_proj_kernel(
    outer, place_ref, x_ref, c_ref, basis_ref, other_hbm, other_basis_hbm, proj_ref, *rest
):
    *send_refs, other_ref, other_basis_ref, sems = rest
    step, last = pl.program_id(0), pl.num_programs(0) - 1

    def copies():
        pieces = sems.shape[0] - 1
        rows = other_ref.shape[0] // pieces
        return [
            pltpu.make_async_copy(
                other_hbm.at[pl.ds(i * rows, rows), :],
                other_ref.at[pl.ds(i * rows, rows), :],
                sems.at[i],
            )
            for i in range(pieces)
        ] + [pltpu.make_async_copy(other_basis_hbm, other_basis_ref, sems.at[pieces])]

    finish = fetch(step, last, copies)
    y = jnp.dot(x_ref[...], basis_ref[...], preferred_element_type=F32)
    high, low = split_pair(y.T)
    part = jnp.dot(high, c_ref[...], preferred_element_type=F32) + jnp.dot(
        low, c_ref[...], preferred_element_type=F32
    )

    @pl.when(step == 0)
    def _():
        proj_ref[...] = part

    @pl.when(step > 0)
    def _():
        proj_ref[...] += part

    @pl.when(step == last)
    def _():
        write_sends(place_ref, outer, proj_ref, send_refs)

    finish()


def sends_shape(rank, cols):
    _, inner = groups_of("fs")
    return [jax.ShapeDtypeStruct((rank // inner, cols), F32)] * (inner - 1)


def value_proj(place, x, c, basis, other, other_basis):
    tokens, width = x.shape
    rank, cols = basis.shape[1], c.shape[1]
    block = min(512, tokens)
    outer, inner = groups_of("fs")
    vmem = pl.BlockSpec(memory_space=pltpu.VMEM)
    hbm = pl.BlockSpec(memory_space=pl.ANY)
    return pl.pallas_call(
        functools.partial(value_proj_kernel, outer),
        grid=(tokens // block,),
        out_shape=[jax.ShapeDtypeStruct((rank, cols), F32)]
        + sends_shape(rank, cols)
        + [pltpu.VMEM(other.shape, BF16), pltpu.VMEM(other_basis.shape, BF16)],
        in_specs=[
            pl.BlockSpec(memory_space=pltpu.SMEM),
            pl.BlockSpec((block, width), lambda t: (t, 0)),
            pl.BlockSpec((block, cols), lambda t: (t, 0)),
            pl.BlockSpec((width, rank), lambda t: (0, 0)),
            hbm,
            hbm,
        ],
        out_specs=[pl.BlockSpec((rank, cols), lambda t: (0, 0))]
        + [pl.BlockSpec((rank // inner, cols), lambda t: (0, 0))] * (inner - 1)
        + [vmem, vmem],
        scratch_shapes=[pltpu.SemaphoreType.DMA((5,))],
        cost_estimate=pl.CostEstimate(
            flops=2 * tokens * rank * (width + 2 * cols),
            bytes_accessed=2 * tokens * (2 * width + cols),
            transcendentals=0,
        ),
        compiler_params=pltpu.CompilerParams(vmem_limit_bytes=KERNEL_BYTES),
        name="value_proj",
    )(place, *map(in_hbm, (x, c, basis, other, other_basis)))


def head_copies(sources, targets, sems, start):
    count, _, width = targets[0].shape
    return [
        pltpu.make_async_copy(
            source.at[:, pl.ds((start + j) * width, width)], target.at[j], sems.at[j, i]
        )
        for j in range(count)
        for i, (source, target) in enumerate(zip(sources, targets))
    ]


def low_rank_kernel(half, start, x_ref, basis_ref, *refs):
    if start is not None:
        *sources, high_ref, low_ref, q_ref, k_ref, v_ref, sems = refs
        copies = head_copies(sources, (q_ref, k_ref, v_ref), sems, start)
        for copy in copies:
            copy.start()
    else:
        copies = []
        high_ref, low_ref = refs
    rows = high_ref.shape[0]
    few = min(512, rows)
    for t in range(rows // few):
        y = jnp.dot(
            x_ref[half * rows + t * few : half * rows + (t + 1) * few, :],
            basis_ref[...],
            preferred_element_type=F32,
        )
        high, low = split_pair(y)
        high_ref[t * few : (t + 1) * few, :] = high
        low_ref[t * few : (t + 1) * few, :] = low
    for copy in copies:
        copy.wait()


def heads_in_vmem(count, sources, heads):
    return [
        pltpu.VMEM((count, source.shape[0], source.shape[1] // heads), BF16)
        for source in sources
    ]


def low_rank_rows(half, x, basis, sources, heads, span):
    tokens, width = x.shape[0] // 2, x.shape[1]
    rank = basis.shape[1]
    vmem = pl.BlockSpec(memory_space=pltpu.VMEM)
    fetched = heads_in_vmem(span[1] - span[0], sources, heads) if span else []
    sources = sources if span else []
    return pl.pallas_call(
        functools.partial(low_rank_kernel, half, span[0] if span else None),
        out_shape=[pltpu.VMEM((tokens, rank), BF16)] * 2 + fetched,
        in_specs=[vmem, vmem] + [pl.BlockSpec(memory_space=pl.ANY)] * len(sources),
        out_specs=[vmem] * (2 + len(fetched)),
        scratch_shapes=[pltpu.SemaphoreType.DMA((span[1] - span[0], 3))] if span else [],
        cost_estimate=pl.CostEstimate(
            flops=2 * tokens * rank * width,
            bytes_accessed=2 * tokens * width,
            transcendentals=0,
        ),
        compiler_params=pltpu.CompilerParams(vmem_limit_bytes=KERNEL_BYTES),
        name="low_rank_rows",
    )(x, basis, *map(in_hbm, sources))


def attend_kernel(
    bq, start, outer, inner, after_start, place_ref, lam_ref, gain_ref, q_all, k_all, v_all,
    high_one, low_one, high_two, low_two, *rest
):
    seq = q_all.shape[1]
    width = q_all.shape[2]
    step, last = pl.program_id(0), pl.num_programs(0) - 1
    if after_start is None:
        *rest, e_ref, h_ref, sum_ref = rest
        finish_fetch = lambda: None
    else:
        sources, rest = rest[:3], rest[3:]
        *rest, q_next, k_next, v_next, e_ref, h_ref, sum_ref, sems = rest
        finish_fetch = fetch(
            step, last,
            lambda: head_copies(sources, (q_next, k_next, v_next), sems, after_start),
        )
    proj_ref, *send_refs = rest[-inner:]
    q_ref, k_ref, v_ref = q_all.at[step], k_all.at[step], v_all.at[step]
    half = width // 2
    lam = lam_ref[start + step]
    scale = half**-0.5
    first = lax.broadcasted_iota(jnp.int32, (1, width), 1) < half

    def finish(base, rows, mix, values):
        raw = jnp.dot(mix, values, preferred_element_type=F32)
        square = jnp.mean(raw * raw, axis=-1, keepdims=True)
        normed = raw * lax.rsqrt(square + EPSILON_NORM) * gain_ref[...]
        h_ref[:, pl.ds(base, rows)] = normed.T.astype(BF16)

    keep = lax.broadcasted_iota(jnp.int32, (bq, bq), 1) <= lax.broadcasted_iota(
        jnp.int32, (bq, bq), 0
    )
    keep_both = jnp.concatenate([keep, keep], axis=0)
    for i in range(seq // bq):
        slot = i % 2
        q = q_ref[i * bq : (i + 1) * bq, :]
        zero = jnp.zeros_like(q)
        both = jnp.concatenate(
            [jnp.where(first, q, zero), jnp.where(first, zero, q)], axis=0
        )
        for t in range(i + 1):
            scores = lax.dot_general(
                both, k_ref[t * bq : (t + 1) * bq, :], NT, preferred_element_type=F32
            )
            e = jnp.exp2(scores * (scale * LOG2E))
            if t == i:
                e = jnp.where(keep_both, e, 0.0)
            e_ref[slot, :, t * bq : (t + 1) * bq] = e
            part = e[:, :128]
            for c in range(1, bq // 128):
                part = part + e[:, c * 128 : (c + 1) * 128]
            if t == 0:
                sum_ref[slot] = part
            else:
                sum_ref[slot] += part
        total = jnp.sum(sum_ref[slot], axis=-1, keepdims=True)
        most = total if i == 0 else jnp.maximum(most, total)
        least = total if i == 0 else jnp.minimum(least, total)
        one = 1.0 / total[:bq]
        two = lam / total[bq:]
        n = (i + 1) * bq
        mix = e_ref[slot, :bq, :n] * one - e_ref[slot, bq:, :n] * two
        finish(i * bq, bq, mix.astype(BF16), v_ref[:n, :])
    fine = (jnp.max(most) < 2.0**120) & (jnp.min(least) > 2.0**-60)

    @pl.when(jnp.logical_not(fine))
    def _():
        few = min(128, bq)

        def block(i, carry):
            base = pl.multiple_of(i * few, few)
            q = q_ref[pl.ds(base, few), :]
            zero = jnp.zeros_like(q)
            both = jnp.concatenate(
                [jnp.where(first, q, zero), jnp.where(first, zero, q)], axis=0
            )
            scores = (
                lax.dot_general(both, k_ref[...], NT, preferred_element_type=F32) * scale
            )
            row = lax.broadcasted_iota(jnp.int32, (few, seq), 0)
            keep = lax.broadcasted_iota(jnp.int32, (few, seq), 1) <= base + row
            scores = jnp.where(jnp.concatenate([keep, keep], axis=0), scores, -jnp.inf)
            e_ref[0, : 2 * few, :] = jnp.exp(
                scores - jnp.max(scores, axis=-1, keepdims=True)
            )
            total = jnp.sum(e_ref[0, : 2 * few, :], axis=-1, keepdims=True)
            mix = e_ref[0, :few, :] * (1.0 / total[:few]) - e_ref[0, few : 2 * few, :] * (
                lam / total[few:]
            )
            finish(base, few, mix.astype(BF16), v_ref[...])
            return carry

        lax.fori_loop(0, seq // few, block, 0)

    turned = jnp.zeros((h_ref.shape[0], high_one.shape[1]), F32)
    for part, pair in enumerate(((high_one, low_one), (high_two, low_two))):
        h = h_ref[:, part * (seq // 2) : (part + 1) * (seq // 2)]
        for ref in pair:
            turned = turned + jnp.dot(h, ref[...], preferred_element_type=F32)
    proj_ref[...] = turned.T
    write_sends(place_ref, outer, proj_ref, send_refs)
    finish_fetch()


def attend_heads(
    span, after_span, place, held, sources, mix_lambda, head_gain, pairs, earlier
):
    seq = sources[0].shape[0]
    heads = mix_lambda.shape[0]
    start, stop = span
    count = stop - start
    rank = pairs[0][0].shape[1]
    bq = min(256, seq)
    outer, inner = groups_of("fs")
    vmem = pl.BlockSpec(memory_space=pltpu.VMEM)
    hbm = pl.BlockSpec(memory_space=pl.ANY)
    fetched, extra = [], []
    if after_span:
        ahead = after_span[1] - after_span[0]
        fetched = heads_in_vmem(ahead, sources, heads)
        extra = [pltpu.SemaphoreType.DMA((ahead, 3))]
    sources = list(map(in_hbm, sources)) if after_span else []
    return pl.pallas_call(
        functools.partial(
            attend_kernel, bq, start, outer, inner, after_span and after_span[0]
        ),
        grid=(count,),
        out_shape=[jax.ShapeDtypeStruct((rank, heads * DV), F32)]
        + sends_shape(rank, heads * DV)
        + fetched,
        in_specs=[pl.BlockSpec(memory_space=pltpu.SMEM)] * 2
        + [vmem] * 8
        + [hbm] * (len(sources) + len(earlier)),
        out_specs=[pl.BlockSpec((rank, DV), lambda j: (0, j + start))]
        + [pl.BlockSpec((rank // inner, DV), lambda j: (0, j + start))] * (inner - 1)
        + [vmem] * len(fetched),
        input_output_aliases={10 + len(sources) + i: i for i in range(len(earlier))},
        scratch_shapes=[
            pltpu.VMEM((2, 2 * bq, seq), F32),
            pltpu.VMEM((DV, seq), BF16),
            pltpu.VMEM((2, 2 * bq, 128), F32),
        ]
        + extra,
        cost_estimate=pl.CostEstimate(
            flops=8 * count * seq * seq * DV,
            bytes_accessed=8 * seq * (count * DV + rank),
            transcendentals=count * seq * seq,
        ),
        compiler_params=pltpu.CompilerParams(vmem_limit_bytes=KERNEL_BYTES),
        name="attend_heads",
    )(
        place,
        mix_lambda,
        head_gain.reshape(1, DV),
        *held,
        *pairs[0],
        *pairs[1],
        *sources,
        *earlier,
    )


def out_final_kernel(entries, owner_ref, sum_ref, rank_owner_ref, basis_ref, *refs):
    parts, refs = refs[:4], refs[4:]
    direction, (copy_ref, step_ref, weight_ref, dir_ref, total_ref, held_ref, sems) = (
        refs[:-7], refs[-7:],
    )
    half, rows, share = parts[0].shape
    copies = []
    for p, part in enumerate(parts):
        copy = pltpu.make_async_copy(part, held_ref.at[pl.ds(p * half, half)], sems.at[p])
        copy.start()
        copies.append(copy)
    place_rows(rank_owner_ref, direction, dir_ref)
    high, low = split_pair(dir_ref[...].T)
    total_ref[...] = clip_of(sum_ref, entries) * (
        lax.dot_general(high, basis_ref[...], NT, preferred_element_type=F32)
        + lax.dot_general(low, basis_ref[...], NT, preferred_element_type=F32)
    )
    for p, copy in enumerate(copies):
        copy.wait()
        at = pl.ds((p // 2) * rows, rows)

        def one(a, carry):
            slot = p * half + a
            columns = pl.ds(pl.multiple_of(owner_ref[slot] * share, share), share)
            weight = held_ref[slot] - LEARN_RATE * total_ref[at, columns]
            copy_ref[at, columns] = weight.astype(BF16)
            return carry

        lax.fori_loop(0, half, one, 0)
    own = pl.ds(pl.multiple_of(owner_ref[0] * share, share), share)
    for g in range(2):
        at = pl.ds(g * rows, rows)
        step = total_ref[at, own]
        step_ref[at, :] = step
        weight_ref[at, :] = held_ref[2 * g * half] - LEARN_RATE * step


def out_final(owners, squares, entries, rank_owners, direction, basis, parts):
    half, rows, share = parts[0].shape
    width, rank = basis.shape
    cols = 2 * rows
    smem = pl.BlockSpec(memory_space=pltpu.SMEM)
    vmem = pl.BlockSpec(memory_space=pltpu.VMEM)
    block = jax.ShapeDtypeStruct((cols, share), F32)
    return pl.pallas_call(
        functools.partial(out_final_kernel, entries),
        out_shape=(jax.ShapeDtypeStruct((cols, width), BF16), block, block),
        in_specs=[smem, vmem, smem, vmem]
        + [pl.BlockSpec(memory_space=pl.ANY)] * 4
        + [vmem] * len(direction),
        out_specs=[vmem] * 3,
        scratch_shapes=[
            pltpu.VMEM((rank, cols), F32),
            pltpu.VMEM((cols, width), F32),
            pltpu.VMEM((4 * half, rows, share), F32),
            pltpu.SemaphoreType.DMA((4,)),
        ],
        cost_estimate=pl.CostEstimate(
            flops=4 * rank * cols * width,
            bytes_accessed=6 * cols * width,
            transcendentals=0,
        ),
        compiler_params=pltpu.CompilerParams(vmem_limit_bytes=VMEM_BYTES),
        name="out_final",
    )(owners, squares, rank_owners, basis, *parts, *direction)


def place_rows(owner_ref, parts, out_ref):
    blocks = owner_ref.shape[0] // len(parts)
    rows = parts[0].shape[0] // blocks
    for p, part in enumerate(parts):
        for a in range(blocks):
            at = pl.multiple_of(owner_ref[p * blocks + a] * rows, rows)
            out_ref[pl.ds(at, rows), :] = part[a * rows : (a + 1) * rows, :]


def clip_of(total_ref, entries):
    total = jnp.sum(
        jnp.sum(total_ref[...], axis=0, keepdims=True), axis=1, keepdims=True
    )
    return jnp.minimum(1.0, CLIP_RMS * math.sqrt(entries) / jnp.sqrt(total))


def value_final_kernel(
    entries, me_ref, sum_ref, owner_ref, basis_ref, old_ref, *refs
):
    parts, (step_ref, weight_ref, copy_ref, dir_ref) = refs[:-4], refs[-4:]
    place_rows(owner_ref, parts, dir_ref)
    high, low = split_pair(dir_ref[...])
    total = jnp.dot(basis_ref[...], high, preferred_element_type=F32) + jnp.dot(
        basis_ref[...], low, preferred_element_type=F32
    )
    step = clip_of(sum_ref, entries) * total
    weight = old_ref[...] - LEARN_RATE * step
    step_ref[...] = step
    weight_ref[...] = weight
    copy_ref[...] = weight.astype(BF16)


def value_final(me, squares, entries, owners, direction, basis, old):
    rows, cols = old.shape
    rank = basis.shape[1]
    block = jax.ShapeDtypeStruct((rows, cols), F32)
    whole = lambda shape: pl.BlockSpec(shape, lambda i, me: (0, 0))
    smem = pl.BlockSpec(memory_space=pltpu.SMEM)
    grid_spec = pltpu.PrefetchScalarGridSpec(
        num_scalar_prefetch=1,
        grid=(1,),
        in_specs=[
            whole(squares.shape),
            smem,
            pl.BlockSpec((rows, rank), lambda i, me: (me[0], 0)),
            whole((rows, cols)),
        ]
        + [whole(part.shape) for part in direction],
        out_specs=[whole((rows, cols))] * 3,
        scratch_shapes=[pltpu.VMEM((rank, cols), F32)],
    )
    return pl.pallas_call(
        functools.partial(value_final_kernel, entries),
        grid_spec=grid_spec,
        out_shape=(block, block, jax.ShapeDtypeStruct((rows, cols), BF16)),
        cost_estimate=pl.CostEstimate(
            flops=4 * rank * cols * rows,
            bytes_accessed=14 * old.size,
            transcendentals=0,
        ),
        compiler_params=pltpu.CompilerParams(vmem_limit_bytes=14 * 2**20),
    name="value_final",
    )(me.reshape(1), squares, owners, basis, old, *direction)


def fold(place, part, arrived, groups, rows):
    cols = part.shape[1]
    vmem = pl.BlockSpec(memory_space=pltpu.VMEM)
    return pl.pallas_call(
        functools.partial(fold_kernel, len(arrived)),
        out_shape=[jax.ShapeDtypeStruct((rows, cols), F32)] * groups,
        in_specs=[pl.BlockSpec(memory_space=pltpu.SMEM)] + [vmem] * (1 + len(arrived)),
        out_specs=[vmem] * groups,
        cost_estimate=pl.CostEstimate(
            flops=part.size, bytes_accessed=8 * part.size, transcendentals=0
        ),
        compiler_params=pltpu.CompilerParams(vmem_limit_bytes=6 * 2**20),
        name="fold",
    )(place, part, *arrived)


def fold_kernel(count, place_ref, part_ref, *refs):
    arrived, outs = refs[:count], refs[count:]
    rows = outs[0].shape[0]
    for d, out in enumerate(outs):
        member = place_ref[2] ^ d
        at = pl.multiple_of((member * place_ref[1] + place_ref[0]) * rows, rows)
        total = part_ref[pl.ds(at, rows), :]
        for other in arrived:
            total = total + other[pl.ds(pl.multiple_of(member * rows, rows), rows), :]
        out[...] = total


def square_kernel(*refs):
    parts, out_ref = refs[:-1], refs[-1]
    sums = []
    for part in parts:
        rows, cols = part.shape
        total = jnp.zeros((8, 128), F32)
        for r in range(rows // 8):
            for c in range(cols // 128):
                x = part[r * 8 : (r + 1) * 8, c * 128 : (c + 1) * 128]
                total = total + x * x
        sums.append(total)
    while len(sums) > 1:
        sums = [a + b for a, b in zip(sums[::2], sums[1::2])]
    out_ref[...] = sums[0]


def square_sums(parts):
    vmem = pl.BlockSpec(memory_space=pltpu.VMEM)
    return pl.pallas_call(
        square_kernel,
        out_shape=jax.ShapeDtypeStruct((8, 128), F32),
        in_specs=[vmem] * len(parts),
        out_specs=vmem,
        cost_estimate=pl.CostEstimate(
            flops=2 * len(parts) * parts[0].size,
            bytes_accessed=4 * len(parts) * parts[0].size,
            transcendentals=0,
        ),
        compiler_params=pltpu.CompilerParams(vmem_limit_bytes=4 * 2**20),
        name="square_sums",
    )(*parts)


def assemble_kernel(owner_ref, *refs):
    parts, out_ref = refs[:4], refs[4]
    half, rows, _ = parts[0].shape
    for p, part in enumerate(parts):
        def one(a, carry):
            at = pl.multiple_of(owner_ref[p * half + a] * (2 * rows) + (p // 2) * rows, rows)
            out_ref[pl.ds(at, rows), :] = part[a]
            return carry

        lax.fori_loop(0, half, one, 0)


def assemble(owners, parts):
    half, rows, cols = parts[0].shape
    vmem = pl.BlockSpec(memory_space=pltpu.VMEM)
    return pl.pallas_call(
        assemble_kernel,
        out_shape=jax.ShapeDtypeStruct((4 * half * rows, cols), parts[0].dtype),
        in_specs=[pl.BlockSpec(memory_space=pltpu.SMEM)] + [vmem] * 4,
        out_specs=vmem,
        cost_estimate=pl.CostEstimate(
            flops=0, bytes_accessed=16 * half * rows * cols, transcendentals=0
        ),
        compiler_params=pltpu.CompilerParams(vmem_limit_bytes=VMEM_BYTES),
        name="assemble",
    )(owners, *parts)


def swap(x, axis, bit):
    n = lax.axis_size(axis)
    return lax.ppermute(x, axis, [(i, i ^ bit) for i in range(n)])


def bits_down(n):
    bits = [1 << b for b in range(n.bit_length() - 1)]
    return bits[::-1]


def groups_of(axis):
    n = lax.axis_size(axis)
    outer = min(4, n)
    return outer, n // outer


def reduce_scatter(place, x, sends, axis):
    outer, inner = groups_of(axis)
    rows = x.shape[0] // (outer * inner)
    arrived = [swap(send, axis, d) for d, send in enumerate(sends, 1)]
    sums = fold(place, x, arrived, outer, rows)
    total = sums[0]
    for d in range(1, outer):
        total = total + swap(sums[d], axis, d * inner)
    return total


def gather_and_square(x):
    axis = "fs"
    outer, inner = groups_of(axis)
    near = [x] + [swap(x, axis, d * inner) for d in range(1, outer)]
    squares = square_sums(near)
    near = jnp.concatenate(near, axis=0)
    parts = [near] + [swap(near, axis, d) for d in range(1, inner)]
    away = [p ^ (d * inner) for p in range(inner) for d in range(outer)]
    owners = jnp.array(away, jnp.int32) ^ lax.axis_index(axis)
    squares = sum_over(squares, "tp", lax.axis_size("tp"))
    squares = sum_over(squares, axis, inner)
    return parts, owners, squares, x.size * lax.axis_size(axis) * lax.axis_size("tp")


def gather_by_distance(x, axis):
    bits = bits_down(lax.axis_size(axis))
    x, other = lax.optimization_barrier((x, swap(x, axis, bits[0])))
    rows = x.shape[0] // 2
    parts, owners = [], []
    for g, order in enumerate((bits[:0:-1], bits[1:])):
        cut = slice(g * rows, (g + 1) * rows)
        piece = jnp.stack([x[cut], other[cut]])
        away = [0, bits[0]]
        for bit in order[:-1]:
            piece = jnp.concatenate([piece, swap(piece, axis, bit)])
            away = away + [a ^ bit for a in away]
        last = order[-1]
        parts += [piece, swap(piece, axis, last)]
        owners += away + [a ^ last for a in away]
    return parts, jnp.array(owners, jnp.int32) ^ lax.axis_index(axis)


def sum_over(x, axis, group):
    for bit in bits_down(group)[::-1]:
        x = x + swap(x, axis, bit)
    return x


def moment_step(proj, first, second):
    new_first = BETA_ONE * first + (1.0 - BETA_ONE) * proj
    new_second = BETA_TWO * second + (1.0 - BETA_TWO) * proj * proj
    direction = new_first / (jnp.sqrt(new_second) + EPSILON_ADAM)
    return (new_first, new_second, direction)


def body(
    query_rows,
    key_rows,
    value_rows,
    mix_lambda,
    head_gain,
    out_cotangent,
    layer_input,
    value_cotangent,
    out_weight,
    value_weight,
    out_basis,
    value_basis,
    out_first,
    out_second,
    value_first,
    value_second,
):
    me = lax.axis_index("fs")
    parts, owners = gather_by_distance(out_weight, "fs")

    inner = groups_of("fs")[1]
    place = jnp.stack([me % inner, jnp.int32(inner), me // inner]).astype(jnp.int32)
    value_part, *value_sends, cotangent, basis = value_proj(
        place, layer_input, value_cotangent, value_basis, out_cotangent, out_basis
    )
    value_sum = reduce_scatter(place, value_part, value_sends, "fs")
    new_value_first, new_value_second, value_dir = moment_step(
        value_sum, value_first, value_second
    )
    value_dirs, value_owners, *value_squares = gather_and_square(value_dir)
    value_step, new_value_weight, value_rounded = value_final(
        me, *value_squares, value_owners, value_dirs, value_basis, value_weight
    )
    value_copy = assemble(owners, gather_by_distance(value_rounded, "fs")[0])

    heads = mix_lambda.shape[0]
    sources = [query_rows, key_rows, value_rows]
    cuts = sorted({0, heads // 4, heads // 2, heads})
    spans = list(zip(cuts[:-1], cuts[1:])) + [None]
    pair_one = low_rank_rows(0, cotangent, basis, sources, heads, None)
    high, low, *held = low_rank_rows(1, cotangent, basis, sources, heads, spans[0])
    out_parts = []
    for call, span in enumerate(spans[:-1]):
        outs = attend_heads(
            span, spans[call + 1], place, held, sources, mix_lambda, head_gain,
            (pair_one, (high, low)), out_parts,
        )
        inner = groups_of("fs")[1]
        out_parts, held = list(outs[:inner]), outs[inner:]
    out_sum = reduce_scatter(place, out_parts[0], out_parts[1:], "fs")
    new_out_first, new_out_second, out_dir = moment_step(out_sum, out_first, out_second)
    out_dirs, out_owners, *out_squares = gather_and_square(out_dir)
    out_copy, out_step, new_out_weight = out_final(
        owners, *out_squares, out_owners, out_dirs, out_basis, parts
    )
    return (
        out_step,
        value_step,
        new_out_weight,
        new_value_weight,
        out_copy,
        value_copy,
        new_out_first,
        new_out_second,
        new_value_first,
        new_value_second,
    )


def solution(mesh):
    split, rows = P("fs", "tp"), P("fs", None)
    placed = (
        split, split, split, P("tp"), P(), rows, rows, split,
        P("tp", "fs"), split, P(), P(), split, split, split, split,
    )
    return jax.shard_map(
        body,
        mesh=mesh,
        in_specs=placed,
        out_specs=(
            P("tp", "fs"), split, P("tp", "fs"), split, P("tp", None), P(None, "tp"),
            split, split, split, split,
        ),
        check_vma=False,
    )
```
